768 devices in a mesh: fs: 96 (over z, y), tp: 8 (over x, core).
Axes of the slice: x: 4, y: 8, z: 12, core: 2. Of those that a mesh axis runs over, the one named last changes fastest.
Arguments:
- cotangent: bfloat16 [61440, 1024], P('fs', 'tp'), may hold values from -6 to 6
- inputs: bfloat16 [61440, 1024], P('fs', 'tp'), may hold values from -6 to 6
- pre_act: bfloat16 [61440, 2112], P('fs'), may hold values from -20 to 20
- w_up: bfloat16 [2112, 1024], P('fs', 'tp'), may hold values from -0.1875 to 0.1875
- w_down: bfloat16 [2112, 1024], P('fs', 'tp'), may hold values from -0.125 to 0.125
Outputs:
- grad_input: bfloat16 [61440, 1024], P('fs', 'tp')
- grad_up: float32 [2112, 1024], P('fs', 'tp')
The draws below stay inside these ranges and needn't reach their ends.
All inputs are finite; a program needn't handle non-finite values.
Results may differ from the reference program's by a relative error of at most 0.0049.
Values may be sent and summed in bfloat16 or wider, within the bound.
A program may use at most 64 MiB of HBM per device.

```python
import jax
import jax.numpy as jnp
from jax import lax

D = 1024
FF = 2112
TOKENS = 61440


def strengthened(drawn, stream_key, source, target, shards_of, factor):
    owner, partner = [(jnp.arange(drawn.shape[position]) // (drawn.shape[position] // shards_of)).reshape([-1 if axis == position else 1 for axis in range(drawn.ndim)]) for position in (source, target)]
    chosen = jax.random.permutation(stream_key, shards_of)[partner]
    strong = (owner == chosen) | (owner == (partner + shards_of // 2) % shards_of)
    return jnp.where(strong, factor * drawn, drawn)


def block_levels(stream_key, shape, pieces, low, largest):
    gain, own = 1.0, jax.random.fold_in(stream_key, 6)
    for dim, parts in pieces:
        draws = jnp.exp(jax.random.uniform(jax.random.fold_in(own, dim), (parts,), jnp.float32, low / len(pieces), largest / len(pieces)))
        gain = gain * jnp.repeat(draws, shape[dim] // parts).reshape([-1 if axis == dim else 1 for axis in range(len(shape))])
    return gain


def bell_draw(key, extent, scale, limit, pieces=(), kind=jnp.bfloat16):
    level = block_levels(key, extent, pieces, -0.22, 0.18) if pieces else 1.0
    result = jax.random.normal(key, extent, jnp.float32) * scale * level
    return jnp.minimum(jnp.maximum(result, -limit), limit).astype(kind)


def gaussian_with(key, shape, deviation, reach, pieces, heavy, kind=jnp.bfloat16):
    drawn = deviation * jax.random.normal(key, shape, jnp.float32)
    if pieces:
        drawn = drawn * block_levels(key, shape, pieces, -0.22, 0.18)
    return jnp.clip(strengthened(drawn, jax.random.fold_in(key, 3), *heavy), -reach, reach).astype(kind)


def setup_inputs(seed: int = 0) -> dict:
    key_of = jax.random.split(jax.random.key(seed), 6)
    return {
        "cotangent": bell_draw(key_of[0], (TOKENS, D), 1.0, 6.0, ((0, 96), (1, 8))),
        "inputs": bell_draw(key_of[1], (TOKENS, D), 1.0, 6.0, ((0, 96), (1, 8))),
        "pre_act": gaussian_with(key_of[2], (TOKENS, FF), 1.0, 20.0, ((0, 96),), (0, 1, 96, 4.75)),
        "w_up": bell_draw(key_of[3], (FF, D), D ** -0.5, 0.1875, ((0, 96), (1, 8))),
        "w_down": bell_draw(key_of[4], (FF, D), FF ** -0.5, 0.125, ((0, 96), (1, 8))),
    }


def reference(cotangent, inputs, pre_act, w_up, w_down):
    grad_hidden = lax.dot_general(cotangent, w_down, (((1,), (1,)), ((), ())), preferred_element_type=jnp.float32)
    grad_pre = (2.0 * grad_hidden * jnp.maximum(pre_act.astype(jnp.float32), 0.0)).astype(jnp.bfloat16)
    grad_input = jnp.dot(grad_pre, w_up, preferred_element_type=jnp.float32).astype(jnp.bfloat16)
    summed = lax.dot_general(grad_pre, inputs, (((0,), (0,)), ((), ())), preferred_element_type=jnp.float32)
    grad_up = summed / jnp.sqrt(jnp.float32(TOKENS))
    return (grad_input, grad_up)
```

```python
import functools
import math

import jax
import jax.numpy as jnp
from jax import lax
from jax.experimental import pallas as pl
from jax.experimental.pallas import tpu as pltpu
from jax.sharding import PartitionSpec as P

MESH = pl.DeviceIdType.MESH
F32, BF16 = jnp.float32, jnp.bfloat16
NX, NY, NZ = 4, 8, 12
LAG_X, LAG_U, LAG_C, LAG_R = 2, 2, 5, 9


def body(
    rows, win,
    cot_ref, inp_ref, pre_hbm, wu_ref, wd_ref,
    gi_ref, gu_ref,
    pre, cotf, inpx, wpad, zd, zu, wdx, wux, pret, gpt, sendy, recvy, sendz, recvz, gisend, girecv,
    loc_sem, y_ss, y_rs, c_ss, c_rs, c_fs, i_ss, i_rs, zd_ss, zd_rs, zu_ss, zu_rs,
    x_ss, x_rs, xf_ss, sib_ss, us_ss, us_rs, ry_ss, ry_rs, rz_ss, rz_rs, g_ss, g_rs,
):
    fs, tp = lax.axis_index("fs"), lax.axis_index("tp")
    z, y = lax.div(fs, NY), lax.rem(fs, NY)
    x, c = lax.div(tp, 2), lax.rem(tp, 2)
    xr, xl, xo = lax.rem(x + 1, NX), lax.rem(x + NX - 1, NX), lax.rem(x + 2, NX)
    zp, zm = lax.rem(z + 1, NZ), lax.rem(z + NZ - 1, NZ)
    half_z = NZ // 2
    sib = x * 2 + 1 - c
    toks = cot_ref.shape[0]
    tok2 = toks // 2

    def copy(src, dst, ss, rs, to_fs, to_tp):
        return pltpu.make_async_remote_copy(
            src_ref=src, dst_ref=dst, send_sem=ss, recv_sem=rs,
            device_id=(to_fs, to_tp), device_id_type=MESH,
        )

    barrier = pltpu.get_barrier_semaphore()

    def greet(to_fs, to_tp):
        pl.semaphore_signal(barrier, inc=1, device_id=(to_fs, to_tp), device_id_type=MESH)

    def at_y(k):
        return lax.rem(y + k, NY)

    for k in range(1, NY):
        greet(z * NY + at_y(k), tp)
    greet(zp * NY + y, tp)
    greet(zm * NY + y, tp)
    for core in range(2):
        greet(fs, xr * 2 + core)
        greet(fs, xl * 2 + core)
    greet(fs, sib)

    load = pltpu.make_async_copy(pre_hbm, pre, loc_sem)
    load.start()

    keep = lax.broadcasted_iota(jnp.int32, (24, rows), 0) == lax.broadcasted_iota(jnp.int32, (24, rows), 1)
    keep = keep.astype(F32).astype(BF16)
    for k, ref in enumerate((wd_ref, wu_ref)):
        padded = jnp.dot(keep, ref[...], preferred_element_type=F32)
        padded = padded.reshape(3, 8, 128).astype(BF16)
        wpad[k] = padded
    zd[z, pl.ds(y * 3, 3)] = wpad[0]
    zu[z, pl.ds(y * 3, 3)] = wpad[1]

    pl.semaphore_wait(barrier, NY - 1 + 2 + 4 + 1)

    def y_send(k, w):
        buf = (zd, zu)[w]
        return copy(
            wpad.at[w], buf.at[z, pl.ds(y * 3, 3)], y_ss.at[w, k], y_rs.at[w, y], z * NY + at_y(k), tp
        )

    for k in range(1, NY):
        y_send(k, 0).start()

    def lanes(tile):
        return pl.ds(pl.multiple_of(tile * 128, 128), 128)

    def c_part(tile, h):
        return cotf.at[pl.ds(h * tok2, tok2), lanes(tile)]

    def c_own(h, way):
        to = (xr * 2 + c, xl * 2 + c, sib)[way]
        return copy(
            cot_ref.at[pl.ds(h * tok2, tok2)], c_part(tp, h), c_ss.at[h, way], c_rs.at[tp, h], fs, to
        )

    def c_fwd(tile, h, to, slot):
        return copy(c_part(tile, h), c_part(tile, h), c_fs.at[slot], c_rs.at[tile, h], fs, to)

    for h in range(2):
        for way in range(2):
            c_own(h if way == 0 else 1 - h, way).start()
    for k in range(1, NY):
        y_send(k, 1).start()
    for h in range(2):
        c_own(h, 2).start()
    send_inp = copy(inp_ref, inpx, i_ss, i_rs, fs, sib)
    send_inp.start()

    cotf[:, lanes(tp)] = cot_ref[...]

    load.wait()

    def turn(bl, carry):
        first = (c * half_z + bl) * (rows * NY)
        start = pl.multiple_of(jnp.minimum(lax.div(first, 128), (pre.shape[1] - win) // 128) * 128, 128)
        iy = lax.broadcasted_iota(jnp.int32, (NY, 24, win), 0)
        ir = lax.broadcasted_iota(jnp.int32, (NY, 24, win), 1)
        ik = lax.broadcasted_iota(jnp.int32, (NY, 24, win), 2)
        pick = (ik + start == first + iy * rows + ir) & (ir < rows)
        pick = pick.astype(F32).reshape(NY * 24, win).astype(BF16)
        part = pre[:, pl.ds(start, win)]
        turned = lax.dot_general(pick, part, (((1,), (1,)), ((), ())), preferred_element_type=F32)
        pret[bl] = (2.0 * jnp.maximum(turned, 0.0)).astype(BF16)
        return carry

    lax.fori_loop(0, half_z, turn, 0)

    def y_recv(k, w):
        ys = at_y(k)
        buf = (zd, zu)[w]
        return copy(
            wpad.at[w], buf.at[z, pl.ds(ys * 3, 3)], y_ss.at[w, k], y_rs.at[w, ys], fs, tp
        )

    def block_of(t, sign):
        s = lax.div(t + 1, 2)
        odd = lax.rem(t, 2) == 1
        return lax.rem(z + NZ + jnp.where(odd, -s, s) * sign, NZ)

    def ring_copy(buf, b, to_z, ss, rs):
        return copy(buf.at[b], buf.at[b], ss, rs.at[b], to_z * NY + y, tp)

    def ring_step(buf, t, sign, ss, rs):
        b = block_of(t, sign)
        up, down = (zp, zm) if sign > 0 else (zm, zp)

        @pl.when(t > 0)
        def _():
            ring_copy(buf, b, zp, ss.at[b], rs).wait_recv()

        @pl.when(t == 0)
        def _():
            ring_copy(buf, b, up, ss.at[NZ], rs).start()

        @pl.when(t < NZ - 2)
        def _():
            to = jnp.where(lax.rem(t, 2) == 1, up, down)
            ring_copy(buf, b, to, ss.at[b], rs).start()

        return b

    def wd_part(tile, bl):
        return wdx.at[tile, bl]

    def x_send(b, way):
        h, bl = lax.div(b, half_z), lax.rem(b, half_z)
        to = (xr, xl)[way] * 2 + h
        return copy(zd.at[b], wd_part(tp, bl), x_ss.at[way, b], x_rs.at[tp, bl], fs, to)

    def sib_send(b):
        bl = lax.rem(b, half_z)
        return copy(zd.at[b], wd_part(tp, bl), sib_ss.at[b], x_rs.at[tp, bl], fs, sib)

    def us_send(b):
        bl = lax.rem(b, half_z)
        return copy(zu.at[b], wux.at[c, bl], us_ss.at[b], us_rs.at[bl], fs, sib)

    def in_half(b):
        return lax.div(b, half_z) == c

    def down_step(t):
        b = ring_step(zd, t, 1, zd_ss, zd_rs)
        for way in range(2):
            x_send(b, way).start()

        @pl.when(jnp.logical_not(in_half(b)))
        def _():
            sib_send(b).start()

        @pl.when(in_half(b))
        def _():
            wdx[tp, lax.rem(b, half_z)] = zd[b]

    def up_step(t):
        b = ring_step(zu, t, -1, zu_ss, zu_rs)

        @pl.when(jnp.logical_not(in_half(b)))
        def _():
            us_send(b).start()

        @pl.when(in_half(b))
        def _():
            wux[c, lax.rem(b, half_z)] = zu[b]

    def x_sides(bl, core):
        even = lax.rem(bl + core, 2) == 0
        return jnp.where(even, xl, xr), jnp.where(even, xr, xl)

    def x_forward(bl, core):
        src, dst = x_sides(bl, core)
        tile = src * 2 + core
        return copy(
            wd_part(tile, bl), wd_part(tile, bl), xf_ss.at[core, bl], x_rs.at[tile, bl], fs, dst * 2 + c
        )

    def x_wait(tile, bl):
        copy(wd_part(tile, bl), wd_part(tile, bl), xf_ss.at[0, 0], x_rs.at[tile, bl], fs, tp).wait_recv()

    def x_step(t):
        b = block_of(t, 1)

        @pl.when(in_half(b))
        def _():
            bl = lax.rem(b, half_z)
            for core in range(2):
                fwd = x_forward(bl, core)
                fwd.wait_recv()
                fwd.start()

    def piece(bl, ky, core):
        yt = at_y(ky)
        b = c * half_z + bl
        return copy(
            sendy.at[bl, core, yt], recvy.at[y, b], ry_ss.at[bl, core, ky], ry_rs.at[y, b],
            z * NY + yt, x * 2 + core,
        )

    def compute_step(t):
        b = block_of(t, 1)

        @pl.when(in_half(b))
        def _():
            bl = lax.rem(b, half_z)
            for core in range(2):
                x_wait(x_sides(bl, core)[1] * 2 + core, bl)
                x_wait(xo * 2 + core, bl)
            x_wait(sib, bl)
            w = jnp.concatenate([wdx[k, bl].reshape(NY * 24, 128) for k in range(2 * NX)], axis=1)
            gh = lax.dot_general(w, cotf[...], (((1,), (1,)), ((), ())), preferred_element_type=F32)
            gp = (gh * pret[bl].astype(F32)).astype(BF16)
            gpt[bl] = gp
            for core in range(2):
                @pl.when(c == core)
                def _():
                    own = jnp.dot(gp, inp_ref[...], preferred_element_type=F32)
                    other = jnp.dot(gp, inpx[...], preferred_element_type=F32)
                    sendy[bl, core] = own.reshape(NY, 3, 8, 128).astype(BF16)
                    sendy[bl, 1 - core] = other.reshape(NY, 3, 8, 128).astype(BF16)
            recvy[y, b] = sendy[bl, c, y]
            for ky in range(1, NY):
                for core in range(2):
                    piece(bl, ky, core).start()
            piece(bl, 0, 1 - c).start()

    def z_piece(b):
        return copy(sendz.at[b], recvz.at[z], rz_ss.at[b], rz_rs.at[z], b * NY + y, tp)

    def reduce_step(t):
        b = block_of(t, 1)
        own = in_half(b)
        for ky in range(NY):
            ys = at_y(ky)
            wait = copy(sendy.at[0, 0, 0], recvy.at[ys, b], ry_ss.at[0, 0, 0], ry_rs.at[ys, b], fs, tp)
            if ky == 0:
                @pl.when(jnp.logical_not(own))
                def _():
                    wait.wait_recv()
            else:
                wait.wait_recv()
        total = recvy[0, b].astype(F32)
        for k in range(1, NY):
            total = total + recvy[k, b].astype(F32)
        sendz[b] = total.astype(BF16)

        @pl.when(t == 0)
        def _():
            recvz[z] = sendz[b]

        @pl.when(t > 0)
        def _():
            z_piece(b).start()

    for k in range(1, NY):
        y_recv(k, 0).wait_recv()
    down_step(0)

    def c_wait(tile, h):
        c_fwd(tile, h, sib, 0).wait_recv()

    def c_step_one():
        for h in range(2):
            left, right = xl * 2 + c, xr * 2 + c
            c_wait(left, h)
            if h == 0:
                c_fwd(left, h, xr * 2 + c, 0).start()
            c_fwd(left, h, sib, 1 + h).start()
            c_wait(right, 1 - h)
            if h == 0:
                c_fwd(right, 1, xl * 2 + c, 3).start()
            c_fwd(right, 1 - h, sib, 4 + h).start()

    def c_step_two():
        far = xo * 2 + c
        for h in range(2):
            c_wait(far, h)
            c_fwd(far, h, sib, 6 + h).start()

    def c_step_three():
        for k in range(NX):
            for h in range(2):
                c_wait(lax.rem(x + k, NX) * 2 + 1 - c, h)
        send_inp.wait_recv()

    def run(t, carry):
        @pl.when((t > 0) & (t < NZ))
        def _():
            down_step(t)

        @pl.when(t == 1)
        def _():
            c_step_one()
            for k in range(1, NY):
                y_recv(k, 1).wait_recv()

        @pl.when(t == 3)
        def _():
            c_step_two()

        @pl.when(t == LAG_C)
        def _():
            c_step_three()

        @pl.when((t >= LAG_X) & (t < NZ + LAG_X))
        def _():
            x_step(t - LAG_X)

        @pl.when((t >= LAG_U) & (t < NZ + LAG_U))
        def _():
            up_step(t - LAG_U)

        @pl.when((t >= LAG_C) & (t < NZ + LAG_C))
        def _():
            compute_step(t - LAG_C)

        @pl.when(t >= LAG_R)
        def _():
            reduce_step(t - LAG_R)

        return carry

    lax.fori_loop(0, NZ + LAG_C, run, 0)

    def up_wait(bl, carry):
        copy(wux.at[0, bl], wux.at[0, bl], us_ss.at[0], us_rs.at[bl], fs, tp).wait_recv()
        return carry

    lax.fori_loop(0, half_z, up_wait, 0)

    def gi_part(core):
        total = None
        for bl in range(half_z):
            gp = jnp.transpose(gpt[bl].astype(F32)).astype(BF16)
            term = jnp.dot(gp, wux[core, bl].reshape(NY * 24, 128), preferred_element_type=F32)
            total = term if total is None else total + term
        return total

    gisend[...] = gi_part(1 - c)
    own_part = gi_part(c)
    send_gi = copy(gisend, girecv, g_ss, g_rs, fs, sib)
    send_gi.start()

    def rest(t, carry):
        reduce_step(t)
        return carry

    lax.fori_loop(NZ + LAG_C - LAG_R, NZ, rest, 0)

    send_gi.wait_recv()
    gi_ref[...] = (own_part + girecv[...]).astype(BF16)

    def z_wait(t, carry):
        b = block_of(t, 1)
        copy(sendz.at[0], recvz.at[b], rz_ss.at[0], rz_rs.at[b], fs, tp).wait_recv()
        return carry

    lax.fori_loop(1, NZ, z_wait, 0)
    total = recvz[0].astype(F32)
    for k in range(1, NZ):
        total = total + recvz[k].astype(F32)
    scale = 1.0 / math.sqrt(toks * NY * NZ)
    gu_ref[...] = total.reshape(24, 128)[:rows] * scale

    for k in range(1, NY):
        for w in range(2):
            y_send(k, w).wait_send()
    for h in range(2):
        for way in range(3):
            c_own(h, way).wait_send()
    for slot in range(8):
        c_fwd(tp, 0, sib, slot).wait_send()
    send_inp.wait_send()
    send_gi.wait_send()

    def drain(t, carry):
        b = block_of(t, 1)
        for buf, ss, rs in ((zd, zd_ss, zd_rs), (zu, zu_ss, zu_rs)):
            @pl.when(t == 0)
            def _():
                ring_copy(buf, b, zp, ss.at[NZ], rs).wait_send()
        bu = block_of(t, -1)

        @pl.when(t < NZ - 2)
        def _():
            ring_copy(zd, b, zp, zd_ss.at[b], zd_rs).wait_send()
            ring_copy(zu, bu, zp, zu_ss.at[bu], zu_rs).wait_send()

        for way in range(2):
            x_send(b, way).wait_send()

        @pl.when(jnp.logical_not(in_half(b)))
        def _():
            sib_send(b).wait_send()
            us_send(b).wait_send()

        @pl.when(t > 0)
        def _():
            z_piece(b).wait_send()

        return carry

    lax.fori_loop(0, NZ, drain, 0)

    def drain_pieces(bl, carry):
        for core in range(2):
            x_forward(bl, core).wait_send()
        for ky in range(1, NY):
            for core in range(2):
                piece(bl, ky, core).wait_send()
        piece(bl, 0, 1 - c).wait_send()
        return carry

    lax.fori_loop(0, half_z, drain_pieces, 0)


def local(cotangent, inputs, pre_act, w_up, w_down):
    toks, cols = cotangent.shape
    rows = w_down.shape[0]
    ff = pre_act.shape[1]
    half = NZ // 2
    hid = 24 * NY
    win = ff - (ff - (rows * NY + 127)) // 128 * 128
    vmem, dma = pltpu.VMEM, pltpu.SemaphoreType.DMA
    blk = (3 * NY, 8, 128)
    kernel = functools.partial(body, rows, win)
    return tuple(
        pl.pallas_call(
            kernel,
            out_shape=(
                jax.ShapeDtypeStruct((toks, cols), BF16),
                jax.ShapeDtypeStruct((rows, cols), F32),
            ),
            in_specs=[
                pl.BlockSpec(memory_space=vmem),
                pl.BlockSpec(memory_space=vmem),
                pl.BlockSpec(memory_space=pl.ANY),
                pl.BlockSpec(memory_space=vmem),
                pl.BlockSpec(memory_space=vmem),
            ],
            out_specs=(pl.BlockSpec(memory_space=vmem), pl.BlockSpec(memory_space=vmem)),
            scratch_shapes=[
                vmem((toks, ff), BF16),
                vmem((toks, 128 * 2 * NX), BF16),
                vmem((toks, 128), BF16),
                vmem((2, 3, 8, 128), BF16),
                vmem((NZ, *blk), BF16),
                vmem((NZ, *blk), BF16),
                vmem((2 * NX, half, *blk), BF16),
                vmem((2, half, *blk), BF16),
                vmem((half, hid, toks), BF16),
                vmem((half, hid, toks), BF16),
                vmem((half, 2, NY, 3, 8, 128), BF16),
                vmem((NY, NZ, 3, 8, 128), BF16),
                vmem((NZ, 3, 8, 128), BF16),
                vmem((NZ, 3, 8, 128), BF16),
                vmem((toks, 128), F32),
                vmem((toks, 128), F32),
                dma,
                dma((2, NY)), dma((2, NY)),
                dma((2, 3)), dma((2 * NX, 2)), dma((8,)),
                dma, dma,
                dma((NZ + 1,)), dma((NZ,)), dma((NZ + 1,)), dma((NZ,)),
                dma((2, NZ)), dma((2 * NX, half)), dma((2, half)), dma((NZ,)), dma((NZ,)), dma((half,)),
                dma((half, 2, NY)), dma((NY, NZ)), dma((NZ,)), dma((NZ,)), dma, dma,
            ],
            compiler_params=pltpu.CompilerParams(collective_id=0, has_side_effects=True),
        )(cotangent, inputs, pre_act, w_up, w_down)
    )


def solution(mesh):
    return jax.shard_map(
        local,
        mesh=mesh,
        in_specs=(P("fs", "tp"), P("fs", "tp"), P("fs", None), P("fs", "tp"), P("fs", "tp")),
        out_specs=(P("fs", "tp"), P("fs", "tp")),
        check_vma=False,
    )
```

```python
import functools
import math

import jax
import jax.numpy as jnp
from jax import lax
from jax.experimental import pallas as pl
from jax.experimental.pallas import tpu as pltpu
from jax.sharding import PartitionSpec as P

MESH = pl.DeviceIdType.MESH
F32, BF16 = jnp.float32, jnp.bfloat16
NX, NY, NZ = 4, 8, 12
LAG_X, LAG_U, LAG_C, LAG_R = 2, 1, 5, 12


def body(
    rows,
    cot_hbm, inp_hbm, pre_hbm, wu_hbm, wd_hbm,
    gi_ref, gu_ref,
    cot_ref, inp_ref, wu_ref, wd_ref, pre, cotf, inpx, wpad, zd, zu, wdx, wux, pret, gpt, sendy, recvy, sendz, recvz, gisend, girecv,
    load_sem, y_ss, y_rs, c_ss, c_rs, i_ss, i_rs, ring_ss, zd_rs, zu_rs,
    x_ss, x_rs, us_rs, ry_ss, ry_rs, rz_ss, rz_rs, g_ss, g_rs,
):
    fs, tp = lax.axis_index("fs"), lax.axis_index("tp")
    z, y = lax.div(fs, NY), lax.rem(fs, NY)
    x, c = lax.div(tp, 2), lax.rem(tp, 2)
    xr, xl, xo = lax.rem(x + 1, NX), lax.rem(x + NX - 1, NX), lax.rem(x + 2, NX)
    zp, zm = lax.rem(z + 1, NZ), lax.rem(z + NZ - 1, NZ)
    half_z = NZ // 2
    sib = x * 2 + 1 - c
    toks = cot_ref.shape[0]
    tok2 = toks // 2
    hid = rows * NY

    def copy(src, dst, ss, rs, to_fs, to_tp):
        return pltpu.make_async_remote_copy(
            src_ref=src, dst_ref=dst, send_sem=ss, recv_sem=rs,
            device_id=(to_fs, to_tp), device_id_type=MESH,
        )

    barrier = pltpu.get_barrier_semaphore()

    def greet(to_fs, to_tp):
        pl.semaphore_signal(barrier, inc=1, device_id=(to_fs, to_tp), device_id_type=MESH)

    def at_y(k):
        return lax.rem(y + k, NY)

    for k in range(1, NY):
        greet(z * NY + at_y(k), tp)
    greet(zp * NY + y, tp)
    greet(zm * NY + y, tp)
    for core in range(2):
        greet(fs, xr * 2 + core)
        greet(fs, xl * 2 + core)
    greet(fs, sib)

    own_pre = pre_hbm.at[pl.ds(c * (half_z * hid), half_z * hid)]
    loads = [
        pltpu.make_async_copy(src, dst, load_sem.at[k])
        for k, (src, dst) in enumerate(
            ((wd_hbm, wd_ref), (wu_hbm, wu_ref), (cot_hbm, cot_ref), (inp_hbm, inp_ref), (own_pre, pre))
        )
    ]
    for load in loads:
        load.start()

    keep = lax.broadcasted_iota(jnp.int32, (24, rows), 0) == lax.broadcasted_iota(jnp.int32, (24, rows), 1)
    keep = keep.astype(F32).astype(BF16)
    for k, ref in enumerate((wd_ref, wu_ref)):
        loads[k].wait()
        padded = jnp.dot(keep, ref[...], preferred_element_type=F32)
        padded = padded.reshape(3, 8, 128).astype(BF16)
        wpad[k] = padded
    zd[z, pl.ds(y * 3, 3)] = wpad[0]
    zu[z, pl.ds(y * 3, 3)] = wpad[1]

    pl.semaphore_wait(barrier, NY - 1 + 2 + 4 + 1)

    def y_send(k, w):
        buf = (zd, zu)[w]
        return copy(
            wpad.at[w], buf.at[z, pl.ds(y * 3, 3)], y_ss, y_rs.at[w], z * NY + at_y(k), tp
        )

    for k in range(1, NY):
        y_send(k, 0).start()

    def lanes(tile):
        return pl.ds(pl.multiple_of(tile * 128, 128), 128)

    def c_part(tile, h):
        return cotf.at[pl.ds(h * tok2, tok2), lanes(tile)]

    def c_own(h, way):
        to = (xr * 2 + c, xl * 2 + c, sib)[way]
        return copy(
            cot_ref.at[pl.ds(h * tok2, tok2)], c_part(tp, h), c_ss, c_rs.at[3 if way == 2 else int(way != h)], fs, to
        )

    def c_fwd(tile, h, to, kind):
        return copy(c_part(tile, h), c_part(tile, h), c_ss, c_rs.at[kind], fs, to)

    def c_wait(kind, parts):
        ref = cotf.at[pl.ds(0, tok2), pl.ds(0, 128 * parts)]
        copy(ref, ref, c_ss, c_rs.at[kind], fs, tp).wait_recv()

    loads[2].wait()
    for h in range(2):
        for way in range(2):
            c_own(h if way == 0 else 1 - h, way).start()
    for k in range(1, NY):
        y_send(k, 1).start()
    for h in range(2):
        c_own(h, 2).start()
    loads[3].wait()
    send_inp = copy(inp_ref, inpx, i_ss, i_rs, fs, sib)
    send_inp.start()

    cotf[:, lanes(tp)] = cot_ref[...]

    loads[4].wait()
    iy = lax.broadcasted_iota(jnp.int32, (NY, 24, hid), 0)
    ir = lax.broadcasted_iota(jnp.int32, (NY, 24, hid), 1)
    ik = lax.broadcasted_iota(jnp.int32, (NY, 24, hid), 2)
    pick = ((ik == iy * rows + ir) & (ir < rows)).astype(F32).reshape(NY * 24, hid).astype(BF16)

    def spread(bl, carry):
        part = pre[pl.ds(pl.multiple_of(bl * hid, 16), hid)]
        part = jnp.dot(pick, part, preferred_element_type=F32)
        pret[bl] = (2.0 * jnp.maximum(part, 0.0)).astype(BF16)
        return carry

    lax.fori_loop(0, half_z, spread, 0)

    def y_wait(w):
        buf = (zd, zu)[w]
        parts = buf.at[0, pl.ds(0, 3 * (NY - 1))]
        copy(parts, parts, y_ss, y_rs.at[w], fs, tp).wait_recv()

    def block_of(t, sign):
        s = lax.div(t + 1, 2)
        odd = lax.rem(t, 2) == 1
        return lax.rem(z + NZ + jnp.where(odd, -s, s) * sign, NZ)

    def ring_copy(buf, b, to_z, rs):
        return copy(buf.at[b], buf.at[b], ring_ss, rs.at[b], to_z * NY + y, tp)

    def ring_step(buf, t, sign, rs):
        b = block_of(t, sign)
        up, down = (zp, zm) if sign > 0 else (zm, zp)

        @pl.when(t > 0)
        def _():
            ring_copy(buf, b, zp, rs).wait_recv()

        @pl.when(t == 0)
        def _():
            ring_copy(buf, b, up, rs).start()

        @pl.when(t < NZ - 2)
        def _():
            to = jnp.where(lax.rem(t, 2) == 1, up, down)
            ring_copy(buf, b, to, rs).start()

        return b

    def wd_part(tile, bl):
        return wdx.at[tile * half_z + bl]

    def via_right(bl, core):
        return lax.rem(bl + core, 2) == 0

    def x_send(b, way):
        h, bl = lax.div(b, half_z), lax.rem(b, half_z)
        to = (xr, xl)[way] * 2 + h
        kind = jnp.where(via_right(bl, c) == (way == 0), 0, 1)
        return copy(zd.at[b], wd_part(tp, bl), x_ss, x_rs.at[kind, bl], fs, to)

    def sib_send(b):
        bl = lax.rem(b, half_z)
        return copy(zd.at[b], wd_part(tp, bl), x_ss, x_rs.at[1, bl], fs, sib)

    def us_send(b):
        bl = lax.rem(b, half_z)
        return copy(zu.at[b], wux.at[c, bl], x_ss, us_rs, fs, sib)

    def in_half(b):
        return lax.div(b, half_z) == c

    def down_step(t):
        b = ring_step(zd, t, 1, zd_rs)
        for way in range(2):
            x_send(b, way).start()

        @pl.when(jnp.logical_not(in_half(b)))
        def _():
            sib_send(b).start()

        @pl.when(in_half(b))
        def _():
            wdx[tp * half_z + lax.rem(b, half_z)] = zd[b]

    def up_step(t):
        b = ring_step(zu, t, -1, zu_rs)

        @pl.when(jnp.logical_not(in_half(b)))
        def _():
            us_send(b).start()

        @pl.when(in_half(b))
        def _():
            wux[c, lax.rem(b, half_z)] = zu[b]

    def x_forward(bl, core):
        right = via_right(bl, core)
        src, dst = jnp.where(right, xl, xr), jnp.where(right, xr, xl)
        part = wd_part(src * 2 + core, bl)
        return copy(part, part, x_ss, x_rs.at[1, bl], fs, dst * 2 + c)

    def x_wait(kind, bl, parts):
        ref = wdx.at[pl.ds(0, parts)]
        copy(ref, ref, x_ss, x_rs.at[kind, bl], fs, tp).wait_recv()

    def x_step(t):
        b = block_of(t, 1)

        @pl.when(in_half(b))
        def _():
            bl = lax.rem(b, half_z)
            x_wait(0, bl, 2)
            for core in range(2):
                x_forward(bl, core).start()

    def piece(bl, ky, core):
        yt = at_y(ky)
        b = c * half_z + bl
        return copy(
            sendy.at[bl, core, yt], recvy.at[b, y], ry_ss, ry_rs.at[b],
            z * NY + yt, x * 2 + core,
        )

    def compute_step(t):
        b = block_of(t, 1)

        @pl.when(in_half(b))
        def _():
            bl = lax.rem(b, half_z)
            x_wait(1, bl, 5)
            w = jnp.concatenate([wdx[k * half_z + bl].reshape(NY * 24, 128) for k in range(2 * NX)], axis=1)
            gh = lax.dot_general(w, cotf[...], (((1,), (1,)), ((), ())), preferred_element_type=F32)
            gp = (gh * pret[bl].astype(F32)).astype(BF16)
            gpt[bl] = gp
            for core in range(2):
                @pl.when(c == core)
                def _():
                    own = jnp.dot(gp, inp_ref[...], preferred_element_type=F32)
                    other = jnp.dot(gp, inpx[...], preferred_element_type=F32)
                    sendy[bl, core] = own.reshape(NY, 3, 8, 128).astype(BF16)
                    sendy[bl, 1 - core] = other.reshape(NY, 3, 8, 128).astype(BF16)
            recvy[b, y] = sendy[bl, c, y]
            for ky in range(1, NY):
                for core in range(2):
                    piece(bl, ky, core).start()
            piece(bl, 0, 1 - c).start()

    def z_piece(b):
        return copy(sendz.at[b], recvz.at[z], rz_ss, rz_rs, b * NY + y, tp)

    def reduce_step(t):
        b = block_of(t, 1)
        own = in_half(b)
        for count, when in ((NY - 1, own), (NY, jnp.logical_not(own))):
            @pl.when(when)
            def _():
                ref = recvy.at[b, pl.ds(0, count)]
                copy(ref, ref, ry_ss, ry_rs.at[b], fs, tp).wait_recv()

        total = recvy[b, 0].astype(F32)
        for k in range(1, NY):
            total = total + recvy[b, k].astype(F32)
        sendz[b] = total.astype(BF16)

        @pl.when(t == 0)
        def _():
            recvz[z] = sendz[b]

        @pl.when(t > 0)
        def _():
            z_piece(b).start()

    left, right = xl * 2 + c, xr * 2 + c

    def c_step_one():
        c_wait(0, 2)
        c_fwd(left, 0, xr * 2 + c, 2).start()
        c_fwd(right, 1, xl * 2 + c, 2).start()
        c_fwd(left, 0, sib, 3).start()
        c_fwd(right, 1, sib, 3).start()

    def c_step_half():
        c_wait(1, 2)
        c_fwd(left, 1, sib, 3).start()
        c_fwd(right, 0, sib, 3).start()

    def c_step_two():
        far = xo * 2 + c
        c_wait(2, 2)
        for h in range(2):
            c_fwd(far, h, sib, 3).start()

    def c_step_three():
        c_wait(3, 2 * NX)
        send_inp.wait_recv()

    c_step_one()
    y_wait(0)
    down_step(0)

    def run(t, carry):
        @pl.when((t > 0) & (t < NZ))
        def _():
            down_step(t)

        @pl.when(t == 1)
        def _():
            c_step_half()
            y_wait(1)

        @pl.when(t == 4)
        def _():
            c_step_two()

        @pl.when(t == LAG_C)
        def _():
            c_step_three()

        @pl.when((t >= LAG_X) & (t < NZ + LAG_X))
        def _():
            x_step(t - LAG_X)

        @pl.when((t >= LAG_U) & (t < NZ + LAG_U))
        def _():
            up_step(t - LAG_U)

        @pl.when((t >= LAG_C) & (t < NZ + LAG_C))
        def _():
            compute_step(t - LAG_C)

        @pl.when(t >= LAG_R)
        def _():
            reduce_step(t - LAG_R)

        return carry

    lax.fori_loop(0, NZ + LAG_C, run, 0)

    copy(wux.at[0], wux.at[0], x_ss, us_rs, fs, tp).wait_recv()

    def gi_part(core):
        total = None
        for bl in range(half_z):
            gp = jnp.transpose(gpt[bl].astype(F32)).astype(BF16)
            term = jnp.dot(gp, wux[core, bl].reshape(NY * 24, 128), preferred_element_type=F32)
            total = term if total is None else total + term
        return total

    gisend[...] = gi_part(1 - c)


    def rest(t, carry):
        reduce_step(t)
        return carry

    lax.fori_loop(NZ + LAG_C - LAG_R, NZ, rest, 0)
    send_gi = copy(gisend, girecv, g_ss, g_rs, fs, sib)
    send_gi.start()
    own_part = gi_part(c)

    send_gi.wait_recv()
    gi_ref[...] = (own_part + girecv[...]).astype(BF16)

    others = sendz.at[pl.ds(0, NZ - 1)]
    copy(others, others, rz_ss, rz_rs, fs, tp).wait_recv()
    total = recvz[0].astype(F32)
    for k in range(1, NZ):
        total = total + recvz[k].astype(F32)
    scale = 1.0 / math.sqrt(toks * NY * NZ)
    gu_ref[...] = total.reshape(24, 128)[:rows] * scale

    send_inp.wait_send()
    send_gi.wait_send()
    copy(others, others, rz_ss, rz_rs, fs, tp).wait_send()
    for ref, ss in (
        (zd.at[pl.ds(0, 2), pl.ds(0, 3 * (NY - 1))], y_ss),
        (cotf.at[:, pl.ds(0, 128 * 7)], c_ss),
        (wdx.at[pl.ds(0, 2 * (NZ - 1))], ring_ss),
        (wdx, x_ss),
        (wdx.at[pl.ds(0, 2 * NY - 1), pl.ds(0, 3 * half_z)], ry_ss),
    ):
        copy(ref, ref, ss, g_rs, fs, tp).wait_send()


def local(cotangent, inputs, pre_act, w_up, w_down):
    toks, cols = cotangent.shape
    rows = w_down.shape[0]
    ff = pre_act.shape[1]
    half = NZ // 2
    hid = 24 * NY
    vmem, dma = pltpu.VMEM, pltpu.SemaphoreType.DMA
    blk = (3 * NY, 8, 128)
    kernel = functools.partial(body, rows)
    return tuple(
        pl.pallas_call(
            kernel,
            out_shape=(
                pltpu.VMEM((toks, cols), BF16),
                pltpu.VMEM((rows, cols), F32),
            ),
            in_specs=[
                pl.BlockSpec(memory_space=pl.ANY),
            ] * 5,
            out_specs=(pl.BlockSpec(memory_space=vmem), pl.BlockSpec(memory_space=vmem)),
            scratch_shapes=[
                vmem((toks, cols), BF16),
                vmem((toks, cols), BF16),
                vmem((rows, cols), BF16),
                vmem((rows, cols), BF16),
                vmem((ff // 2, toks), BF16),
                vmem((toks, 128 * 2 * NX), BF16),
                vmem((toks, 128), BF16),
                vmem((2, 3, 8, 128), BF16),
                vmem((NZ, *blk), BF16),
                vmem((NZ, *blk), BF16),
                vmem((2 * NX * half, *blk), BF16),
                vmem((2, half, *blk), BF16),
                vmem((half, hid, toks), BF16),
                vmem((half, hid, toks), BF16),
                vmem((half, 2, NY, 3, 8, 128), BF16),
                vmem((NZ, NY, 3, 8, 128), BF16),
                vmem((NZ, 3, 8, 128), BF16),
                vmem((NZ, 3, 8, 128), BF16),
                vmem((toks, 128), F32),
                vmem((toks, 128), F32),
                dma((5,)),
                dma, dma((2,)), dma, dma((4,)), dma, dma,
                dma, dma((NZ,)), dma((NZ,)),
                dma, dma((2, half)), dma, dma, dma((NZ,)), dma, dma, dma, dma,
            ],
            compiler_params=pltpu.CompilerParams(collective_id=0, has_side_effects=True),
        )(cotangent, inputs, pre_act.T, w_up, w_down)
    )


def solution(mesh):
    return jax.shard_map(
        local,
        mesh=mesh,
        in_specs=(P("fs", "tp"), P("fs", "tp"), P("fs", None), P("fs", "tp"), P("fs", "tp")),
        out_specs=(P("fs", "tp"), P("fs", "tp")),
        check_vma=False,
    )
```

```python
import functools
import math

import jax
import jax.numpy as jnp
from jax import lax
from jax.experimental import pallas as pl
from jax.experimental.pallas import tpu as pltpu
from jax.sharding import PartitionSpec as P

MESH = pl.DeviceIdType.MESH
F32, BF16 = jnp.float32, jnp.bfloat16
NX, NY, NZ = 4, 8, 12
LAG_X, LAG_C, LAG_R = 2, 5, 12


def body(
    rows,
    cot_hbm, inp_hbm, pre_hbm, wu_hbm, wd_hbm,
    gi_ref, gu_ref,
    cot_ref, inp_ref, wu_ref, wd_ref, pre, cotf, inpx, wpad, zr, wdx, wux, pret, gpt, sendy, recvy, sendz, recvz, gisend, girecv,
    load_sem, y_ss, y_rs, c_ss, c_rs, i_ss, i_rs, ring_ss, zr_rs,
    x_ss, xf_ss, x_rs, us_rs, ry_ss, ry_rs, rz_ss, rz_rs, g_ss, g_rs,
):
    fs, tp = lax.axis_index("fs"), lax.axis_index("tp")
    z, y = lax.div(fs, NY), lax.rem(fs, NY)
    x, c = lax.div(tp, 2), lax.rem(tp, 2)
    xr, xl, xo = lax.rem(x + 1, NX), lax.rem(x + NX - 1, NX), lax.rem(x + 2, NX)
    zp, zm = lax.rem(z + 1, NZ), lax.rem(z + NZ - 1, NZ)
    half_z = NZ // 2
    sib = x * 2 + 1 - c
    toks = cot_ref.shape[0]
    tok2 = toks // 2
    hid = rows * NY

    def copy(src, dst, ss, rs, to_fs, to_tp):
        return pltpu.make_async_remote_copy(
            src_ref=src, dst_ref=dst, send_sem=ss, recv_sem=rs,
            device_id=(to_fs, to_tp), device_id_type=MESH,
        )

    barrier = pltpu.get_barrier_semaphore()

    def greet(to_fs, to_tp):
        pl.semaphore_signal(barrier, inc=1, device_id=(to_fs, to_tp), device_id_type=MESH)

    def at_y(k):
        return lax.rem(y + k, NY)

    for k in range(1, NY):
        for core in range(2):
            greet(z * NY + at_y(k), x * 2 + core)
    greet(zp * NY + y, tp)
    greet(zm * NY + y, tp)
    for core in range(2):
        greet(fs, xr * 2 + core)
        greet(fs, xl * 2 + core)
    greet(fs, sib)

    own_pre = pre_hbm.at[pl.ds(c * (half_z * hid), half_z * hid)]
    loads = [
        pltpu.make_async_copy(src, dst, load_sem.at[k])
        for k, (src, dst) in enumerate(
            ((wd_hbm, wd_ref), (wu_hbm, wu_ref), (cot_hbm, cot_ref), (inp_hbm, inp_ref), (own_pre, pre))
        )
    ]
    for load in loads:
        load.start()

    keep = lax.broadcasted_iota(jnp.int32, (24, rows), 0) == lax.broadcasted_iota(jnp.int32, (24, rows), 1)
    keep = keep.astype(F32).astype(BF16)
    for k, ref in enumerate((wd_ref, wu_ref)):
        loads[k].wait()
        padded = jnp.dot(keep, ref[...], preferred_element_type=F32)
        padded = padded.reshape(3, 8, 128).astype(BF16)
        wpad[k] = padded

    def own_rows(core):
        return zr.at[core * NZ + z, pl.ds(y * 3, 3)]

    own_rows(c)[...] = wpad[1 - c]

    pl.semaphore_wait(barrier, 2 * (NY - 1) + 2 + 4 + 1)

    def y_send(k, w):
        return copy(wpad.at[w], own_rows(c), y_ss, y_rs, z * NY + at_y(k), x * 2 + 1 - w)

    def y_send_sib():
        return copy(wpad.at[c], own_rows(c), y_ss, y_rs, fs, sib)

    for k in range(1, NY):
        y_send(k, 0).start()
    y_send_sib().start()

    def lanes(tile):
        return pl.ds(pl.multiple_of(tile * 128, 128), 128)

    def c_part(tile, h):
        return cotf.at[pl.ds(h * tok2, tok2), lanes(tile)]

    def c_own(h, way):
        to = (xr * 2 + c, xl * 2 + c, sib)[way]
        return copy(
            cot_ref.at[pl.ds(h * tok2, tok2)], c_part(tp, h), c_ss, c_rs.at[3 if way == 2 else int(way != h)], fs, to
        )

    def c_fwd(tile, h, to, kind):
        return copy(c_part(tile, h), c_part(tile, h), c_ss, c_rs.at[kind], fs, to)

    def c_wait(kind, parts):
        ref = cotf.at[pl.ds(0, tok2), pl.ds(0, 128 * parts)]
        copy(ref, ref, c_ss, c_rs.at[kind], fs, tp).wait_recv()

    loads[2].wait()
    for h in range(2):
        for way in range(2):
            c_own(h if way == 0 else 1 - h, way).start()
    for k in range(1, NY):
        y_send(k, 1).start()
    for h in range(2):
        c_own(h, 2).start()
    loads[3].wait()
    send_inp = copy(inp_ref, inpx, i_ss, i_rs, fs, sib)
    send_inp.start()

    cotf[:, lanes(tp)] = cot_ref[...]

    loads[4].wait()
    iy = lax.broadcasted_iota(jnp.int32, (NY, 24, hid), 0)
    ir = lax.broadcasted_iota(jnp.int32, (NY, 24, hid), 1)
    ik = lax.broadcasted_iota(jnp.int32, (NY, 24, hid), 2)
    pick = ((ik == iy * rows + ir) & (ir < rows)).astype(F32).reshape(NY * 24, hid).astype(BF16)

    def spread(bl, carry):
        part = pre[pl.ds(pl.multiple_of(bl * hid, 16), hid)]
        part = jnp.dot(pick, part, preferred_element_type=F32)
        pret[bl] = (2.0 * jnp.maximum(part, 0.0)).astype(BF16)
        return carry

    lax.fori_loop(0, half_z, spread, 0)

    def y_parts():
        ref = zr.at[pl.ds(0, 3), pl.ds(0, 2 * NY - 1)]
        return copy(ref, ref, y_ss, y_rs, fs, tp)

    def block_of(t, sign):
        s = lax.div(t + 1, 2)
        odd = lax.rem(t, 2) == 1
        return lax.rem(z + NZ + jnp.where(odd, -s, s) * sign, NZ)

    ring_sign = jnp.where(c == 1, 1, -1)
    ring_up, ring_down = jnp.where(c == 1, zp, zm), jnp.where(c == 1, zm, zp)

    def ring_copy(slot, to_z):
        return copy(zr.at[slot], zr.at[slot], ring_ss, zr_rs.at[slot], to_z * NY + y, tp)

    def ring_step(t, slot):
        @pl.when(t > 0)
        def _():
            ring_copy(slot, zp).wait_recv()

        @pl.when(t == 0)
        def _():
            ring_copy(slot, ring_up).start()

        @pl.when(t < NZ - 2)
        def _():
            ring_copy(slot, jnp.where(lax.rem(t, 2) == 1, ring_up, ring_down)).start()

    def wd_part(tile, bl):
        return wdx.at[tile * half_z + bl]

    def via_right(bl, core):
        return lax.rem(bl + core, 2) == 0

    def x_send(k, b, way):
        h, bl = lax.div(b, half_z), lax.rem(b, half_z)
        to = (xr, xl)[way] * 2 + h
        kind = jnp.where(via_right(bl, k) == (way == 0), 0, 1)
        return copy(zr.at[k * NZ + b], wd_part(x * 2 + k, bl), x_ss, x_rs.at[kind, bl], fs, to)

    def in_half(b):
        return lax.div(b, half_z) == c

    def gather_step(t, carry):
        b = block_of(t, ring_sign)
        bl = lax.rem(b, half_z)
        for k in range(2):
            slot = k * NZ + b
            ring_step(t, slot)

            @pl.when(c == 1)
            def _():
                for way in range(2):
                    x_send(k, b, way).start()

                @pl.when(in_half(b))
                def _():
                    wdx[(x * 2 + k) * half_z + bl] = zr[slot]

                @pl.when(jnp.logical_not(in_half(b)))
                def _():
                    copy(zr.at[slot], wd_part(x * 2 + k, bl), xf_ss, x_rs.at[1, bl], fs, sib).start()

            @pl.when(c == 0)
            def _():
                @pl.when(in_half(b))
                def _():
                    wux[k * half_z + bl] = zr[slot]

                @pl.when(jnp.logical_not(in_half(b)))
                def _():
                    copy(zr.at[slot], wux.at[k * half_z + bl], xf_ss, us_rs, fs, sib).start()

        return carry

    def x_forward(bl, core):
        right = via_right(bl, core)
        src, dst = jnp.where(right, xl, xr), jnp.where(right, xr, xl)
        part = wd_part(src * 2 + core, bl)
        return copy(part, part, xf_ss, x_rs.at[1, bl], fs, dst * 2 + c)

    def x_wait(kind, bl, parts):
        ref = wdx.at[pl.ds(0, parts)]
        copy(ref, ref, x_ss, x_rs.at[kind, bl], fs, tp).wait_recv()

    def x_step(t):
        b = block_of(t, 1)

        @pl.when(in_half(b))
        def _():
            bl = lax.rem(b, half_z)
            x_wait(0, bl, 2)
            for core in range(2):
                x_forward(bl, core).start()

    def piece(bl, ky, core):
        yt = at_y(ky)
        b = c * half_z + bl
        return copy(
            sendy.at[bl, core, yt], recvy.at[b, y], ry_ss, ry_rs.at[b],
            z * NY + yt, x * 2 + core,
        )

    def compute_step(t):
        b = block_of(t, 1)

        @pl.when(in_half(b))
        def _():
            bl = lax.rem(b, half_z)
            for core, parts in ((0, 6), (1, 4)):
                @pl.when(c == core)
                def _():
                    x_wait(1, bl, parts)

            w = jnp.concatenate([wdx[k * half_z + bl].reshape(NY * 24, 128) for k in range(2 * NX)], axis=1)
            gh = lax.dot_general(w, cotf[...], (((1,), (1,)), ((), ())), preferred_element_type=F32)
            gp = (gh * pret[bl].astype(F32)).astype(BF16)
            gpt[bl] = gp
            for core in range(2):
                @pl.when(c == core)
                def _():
                    own = jnp.dot(gp, inp_ref[...], preferred_element_type=F32)
                    other = jnp.dot(gp, inpx[...], preferred_element_type=F32)
                    sendy[bl, core] = own.reshape(NY, 3, 8, 128).astype(BF16)
                    sendy[bl, 1 - core] = other.reshape(NY, 3, 8, 128).astype(BF16)
            recvy[b, y] = sendy[bl, c, y]
            for ky in range(1, NY):
                for core in range(2):
                    piece(bl, ky, core).start()
            piece(bl, 0, 1 - c).start()

    def z_piece(b):
        return copy(sendz.at[b], recvz.at[z], rz_ss, rz_rs, b * NY + y, tp)

    def reduce_step(t):
        b = block_of(t, 1)
        own = in_half(b)
        for count, when in ((NY - 1, own), (NY, jnp.logical_not(own))):
            @pl.when(when)
            def _():
                ref = recvy.at[b, pl.ds(0, count)]
                copy(ref, ref, ry_ss, ry_rs.at[b], fs, tp).wait_recv()

        total = recvy[b, 0].astype(F32)
        for k in range(1, NY):
            total = total + recvy[b, k].astype(F32)
        sendz[b] = total.astype(BF16)

        @pl.when(t == 0)
        def _():
            recvz[z] = sendz[b]

        @pl.when(t > 0)
        def _():
            z_piece(b).start()

    left, right = xl * 2 + c, xr * 2 + c

    def c_step_one():
        c_wait(0, 2)
        c_fwd(left, 0, xr * 2 + c, 2).start()
        c_fwd(right, 1, xl * 2 + c, 2).start()
        c_fwd(left, 0, sib, 3).start()
        c_fwd(right, 1, sib, 3).start()

    def c_step_half():
        c_wait(1, 2)
        c_fwd(left, 1, sib, 3).start()
        c_fwd(right, 0, sib, 3).start()

    def c_step_two():
        far = xo * 2 + c
        c_wait(2, 2)
        for h in range(2):
            c_fwd(far, h, sib, 3).start()

    def c_step_three():
        c_wait(3, 2 * NX)
        send_inp.wait_recv()

    c_step_one()
    y_parts().wait_recv()

    def run(t, carry):
        hop = lax.div(2 * t - 2 + 4, 5)
        due = (t >= 1) & (lax.div(5 * hop, 2) == t - 1)
        first = jnp.where(c == 1, jnp.minimum(t, NZ), jnp.maximum(2 * hop - 1, 0))
        last = jnp.where(c == 1, t + 1, jnp.where(due, 2 * hop + 1, 0))
        lax.fori_loop(first, jnp.minimum(last, NZ), gather_step, 0)

        @pl.when(t == 1)
        def _():
            c_step_half()

        @pl.when(t == 3)
        def _():
            c_step_two()

        @pl.when(t == LAG_C)
        def _():
            c_step_three()

        @pl.when((t >= LAG_X) & (t < NZ + LAG_X))
        def _():
            x_step(t - LAG_X)

        @pl.when((t >= LAG_C) & (t < NZ + LAG_C))
        def _():
            compute_step(t - LAG_C)

        @pl.when((t >= LAG_R) & (t < NZ + LAG_R))
        def _():
            reduce_step(t - LAG_R)

        return carry

    lax.fori_loop(0, NZ + LAG_C, run, 0)

    @pl.when(c == 1)
    def _():
        copy(wux, wux, x_ss, us_rs, fs, tp).wait_recv()

    def gi_part(core):
        total = None
        for bl in range(half_z):
            gp = jnp.transpose(gpt[bl].astype(F32)).astype(BF16)
            term = jnp.dot(gp, wux[core * half_z + bl].reshape(NY * 24, 128), preferred_element_type=F32)
            total = term if total is None else total + term
        return total

    gisend[...] = gi_part(1 - c)


    def rest(t, carry):
        reduce_step(t)
        return carry

    lax.fori_loop(NZ + LAG_C - LAG_R, NZ, rest, 0)
    send_gi = copy(gisend, girecv, g_ss, g_rs, fs, sib)
    send_gi.start()
    own_part = gi_part(c)

    send_gi.wait_recv()
    gi_ref[...] = (own_part + girecv[...]).astype(BF16)

    others = sendz.at[pl.ds(0, NZ - 1)]
    copy(others, others, rz_ss, rz_rs, fs, tp).wait_recv()
    total = recvz[0].astype(F32)
    for k in range(1, NZ):
        total = total + recvz[k].astype(F32)
    scale = 1.0 / math.sqrt(toks * NY * NZ)
    gu_ref[...] = total.reshape(24, 128)[:rows] * scale

    send_inp.wait_send()
    send_gi.wait_send()
    copy(others, others, rz_ss, rz_rs, fs, tp).wait_send()
    for ref, ss in (
        (zr.at[pl.ds(0, 3), pl.ds(0, 2 * NY - 1)], y_ss),
        (cotf.at[:, pl.ds(0, 128 * 7)], c_ss),
        (wdx.at[pl.ds(0, 2 * (NZ - 1))], ring_ss),
        (wdx.at[pl.ds(0, 4 * half_z)], xf_ss),
        (wdx.at[pl.ds(0, 2 * NY - 1), pl.ds(0, 3 * half_z)], ry_ss),
    ):
        copy(ref, ref, ss, g_rs, fs, tp).wait_send()

    @pl.when(c == 1)
    def _():
        copy(wdx, wdx, x_ss, g_rs, fs, tp).wait_send()


def local(cotangent, inputs, pre_act, w_up, w_down):
    toks, cols = cotangent.shape
    rows = w_down.shape[0]
    ff = pre_act.shape[1]
    half = NZ // 2
    hid = 24 * NY
    vmem, dma = pltpu.VMEM, pltpu.SemaphoreType.DMA
    blk = (3 * NY, 8, 128)
    kernel = functools.partial(body, rows)
    return tuple(
        pl.pallas_call(
            kernel,
            out_shape=(
                pltpu.VMEM((toks, cols), BF16),
                pltpu.VMEM((rows, cols), F32),
            ),
            in_specs=[
                pl.BlockSpec(memory_space=pl.ANY),
            ] * 5,
            out_specs=(pl.BlockSpec(memory_space=vmem), pl.BlockSpec(memory_space=vmem)),
            scratch_shapes=[
                vmem((toks, cols), BF16),
                vmem((toks, cols), BF16),
                vmem((rows, cols), BF16),
                vmem((rows, cols), BF16),
                vmem((ff // 2, toks), BF16),
                vmem((toks, 128 * 2 * NX), BF16),
                vmem((toks, 128), BF16),
                vmem((2, 3, 8, 128), BF16),
                vmem((2 * NZ, *blk), BF16),
                vmem((2 * NX * half, *blk), BF16),
                vmem((2 * half, *blk), BF16),
                vmem((half, hid, toks), BF16),
                vmem((half, hid, toks), BF16),
                vmem((half, 2, NY, 3, 8, 128), BF16),
                vmem((NZ, NY, 3, 8, 128), BF16),
                vmem((NZ, 3, 8, 128), BF16),
                vmem((NZ, 3, 8, 128), BF16),
                vmem((toks, 128), F32),
                vmem((toks, 128), F32),
                dma((5,)),
                dma, dma, dma, dma((4,)), dma, dma,
                dma, dma((2 * NZ,)),
                dma, dma, dma((2, half)), dma, dma, dma((NZ,)), dma, dma, dma, dma,
            ],
            compiler_params=pltpu.CompilerParams(collective_id=0, has_side_effects=True),
        )(cotangent, inputs, pre_act.T, w_up, w_down)
    )


def solution(mesh):
    return jax.shard_map(
        local,
        mesh=mesh,
        in_specs=(P("fs", "tp"), P("fs", "tp"), P("fs", None), P("fs", "tp"), P("fs", "tp")),
        out_specs=(P("fs", "tp"), P("fs", "tp")),
        check_vma=False,
    )
```

```python
import functools
import math

import jax
import jax.numpy as jnp
from jax import lax
from jax.experimental import pallas as pl
from jax.experimental.pallas import tpu as pltpu
from jax.sharding import PartitionSpec as P

MESH = pl.DeviceIdType.MESH
F32, BF16 = jnp.float32, jnp.bfloat16
NX, NY, NZ = 4, 8, 12
LAG_X, LAG_C, LAG_R = 3, 6, 13


def body(
    rows,
    cot_hbm, inp_hbm, pre_hbm, wu_hbm, wd_hbm,
    gi_ref, gu_ref,
    cot_ref, inp_ref, wu_ref, wd_ref, pre, cotf, inpx, wpad, zr, wdx, wux, pret, gpt, sendy, recvy, sendz, recvz, gisend, girecv,
    load_sem, y_ss, y_rs, c_ss, c_rs, i_ss, i_rs, ring_ss, zr_rs,
    x_ss, xf_ss, x_rs, us_rs, ry_ss, ry_rs, rz_ss, rz_rs, g_ss, g_rs,
):
    fs, tp = lax.axis_index("fs"), lax.axis_index("tp")
    z, y = lax.div(fs, NY), lax.rem(fs, NY)
    x, c = lax.div(tp, 2), lax.rem(tp, 2)
    xr, xl, xo = lax.rem(x + 1, NX), lax.rem(x + NX - 1, NX), lax.rem(x + 2, NX)
    zp, zm = lax.rem(z + 1, NZ), lax.rem(z + NZ - 1, NZ)
    half_z = NZ // 2
    sib = x * 2 + 1 - c
    toks = cot_ref.shape[0]
    tok2 = toks // 2
    hid = rows * NY

    def copy(src, dst, ss, rs, to_fs, to_tp):
        return pltpu.make_async_remote_copy(
            src_ref=src, dst_ref=dst, send_sem=ss, recv_sem=rs,
            device_id=(to_fs, to_tp), device_id_type=MESH,
        )

    barrier = pltpu.get_barrier_semaphore()

    def greet(to_fs, to_tp):
        pl.semaphore_signal(barrier, inc=1, device_id=(to_fs, to_tp), device_id_type=MESH)

    def at_y(k):
        return lax.rem(y + k, NY)

    for k in range(1, NY):
        for core in range(2):
            greet(z * NY + at_y(k), x * 2 + core)
    greet(zp * NY + y, tp)
    greet(zm * NY + y, tp)
    for core in range(2):
        greet(fs, xr * 2 + core)
        greet(fs, xl * 2 + core)
    greet(fs, sib)

    own_pre = pre_hbm.at[pl.ds(c * (half_z * hid), half_z * hid)]
    loads = [
        pltpu.make_async_copy(src, dst, load_sem.at[k])
        for k, (src, dst) in enumerate(
            ((wd_hbm, wd_ref), (wu_hbm, wu_ref), (cot_hbm, cot_ref), (inp_hbm, inp_ref), (own_pre, pre))
        )
    ]
    for load in loads:
        load.start()

    keep = lax.broadcasted_iota(jnp.int32, (24, rows), 0) == lax.broadcasted_iota(jnp.int32, (24, rows), 1)
    keep = keep.astype(F32).astype(BF16)
    for k, ref in enumerate((wd_ref, wu_ref)):
        loads[k].wait()
        padded = jnp.dot(keep, ref[...], preferred_element_type=F32)
        padded = padded.reshape(3, 8, 128).astype(BF16)
        wpad[k] = padded

    def own_rows(core):
        return zr.at[core * NZ + z, pl.ds(y * 3, 3)]

    own_rows(c)[...] = wpad[1 - c]

    pl.semaphore_wait(barrier, 2 * (NY - 1) + 2 + 4 + 1)

    def y_send(k, w):
        return copy(wpad.at[w], own_rows(c), y_ss, y_rs, z * NY + at_y(k), x * 2 + 1 - w)

    def y_send_sib():
        return copy(wpad.at[c], own_rows(c), y_ss, y_rs, fs, sib)

    for k in range(1, NY):
        y_send(k, 0).start()
    y_send_sib().start()

    def lanes(tile):
        return pl.ds(pl.multiple_of(tile * 128, 128), 128)

    def c_part(tile, h):
        return cotf.at[pl.ds(h * tok2, tok2), lanes(tile)]

    def c_own(h, way):
        to = (xr * 2 + c, xl * 2 + c, sib)[way]
        return copy(
            cot_ref.at[pl.ds(h * tok2, tok2)], c_part(tp, h), c_ss, c_rs.at[3 if way == 2 else int(way != h)], fs, to
        )

    def c_fwd(tile, h, to, kind):
        return copy(c_part(tile, h), c_part(tile, h), c_ss, c_rs.at[kind], fs, to)

    def c_wait(kind, parts):
        ref = cotf.at[pl.ds(0, tok2), pl.ds(0, 128 * parts)]
        copy(ref, ref, c_ss, c_rs.at[kind], fs, tp).wait_recv()

    loads[2].wait()
    for h in range(2):
        for way in range(2):
            c_own(h if way == 0 else 1 - h, way).start()
    for k in range(1, NY):
        y_send(k, 1).start()
    for h in range(2):
        c_own(h, 2).start()
    loads[3].wait()
    send_inp = copy(inp_ref, inpx, i_ss, i_rs, fs, sib)
    send_inp.start()

    cotf[:, lanes(tp)] = cot_ref[...]

    loads[4].wait()
    iy = lax.broadcasted_iota(jnp.int32, (NY, 24, hid), 0)
    ir = lax.broadcasted_iota(jnp.int32, (NY, 24, hid), 1)
    ik = lax.broadcasted_iota(jnp.int32, (NY, 24, hid), 2)
    pick = ((ik == iy * rows + ir) & (ir < rows)).astype(F32).reshape(NY * 24, hid).astype(BF16)

    def spread(bl, carry):
        part = pre[pl.ds(pl.multiple_of(bl * hid, 16), hid)]
        part = jnp.dot(pick, part, preferred_element_type=F32)
        pret[bl] = (2.0 * jnp.maximum(part, 0.0)).astype(BF16)
        return carry

    lax.fori_loop(0, half_z, spread, 0)

    def y_parts():
        ref = zr.at[pl.ds(0, 3), pl.ds(0, 2 * NY - 1)]
        return copy(ref, ref, y_ss, y_rs, fs, tp)

    def block_of(t, sign):
        s = lax.div(t + 1, 2)
        odd = lax.rem(t, 2) == 1
        return lax.rem(z + NZ + jnp.where(odd, -s, s) * sign, NZ)

    ring_sign = jnp.where(c == 1, 1, -1)
    ring_up, ring_down = jnp.where(c == 1, zp, zm), jnp.where(c == 1, zm, zp)

    def ring_copy(slot, to_z):
        return copy(zr.at[slot], zr.at[slot], ring_ss, zr_rs.at[slot], to_z * NY + y, tp)

    def ring_step(t, slot):
        @pl.when(t > 0)
        def _():
            ring_copy(slot, zp).wait_recv()

        @pl.when(t == 0)
        def _():
            ring_copy(slot, ring_up).start()

        @pl.when(t < NZ - 2)
        def _():
            ring_copy(slot, jnp.where(lax.rem(t, 2) == 1, ring_up, ring_down)).start()

    def wd_part(tile, bl):
        return wdx.at[tile * half_z + bl]

    def via_right(bl, core):
        return lax.rem(bl + core, 2) == 0

    def x_send(k, b, way):
        h, bl = lax.div(b, half_z), lax.rem(b, half_z)
        to = (xr, xl)[way] * 2 + h
        kind = jnp.where(via_right(bl, k) == (way == 0), 0, 1)
        return copy(zr.at[k * NZ + b], wd_part(x * 2 + k, bl), x_ss, x_rs.at[kind, bl], fs, to)

    def in_half(b):
        return lax.div(b, half_z) == c

    def gather_step(t, carry):
        b = block_of(t, ring_sign)
        bl = lax.rem(b, half_z)
        for k in range(2):
            slot = k * NZ + b
            ring_step(t, slot)

            @pl.when(c == 1)
            def _():
                for way in range(2):
                    x_send(k, b, way).start()

                @pl.when(in_half(b))
                def _():
                    wdx[(x * 2 + k) * half_z + bl] = zr[slot]

                @pl.when(jnp.logical_not(in_half(b)))
                def _():
                    copy(zr.at[slot], wd_part(x * 2 + k, bl), xf_ss, x_rs.at[1, bl], fs, sib).start()

            @pl.when(c == 0)
            def _():
                @pl.when(in_half(b))
                def _():
                    wux[k * half_z + bl] = zr[slot]

                @pl.when(jnp.logical_not(in_half(b)))
                def _():
                    copy(zr.at[slot], wux.at[k * half_z + bl], xf_ss, us_rs, fs, sib).start()

        return carry

    def x_forward(bl, core):
        right = via_right(bl, core)
        src, dst = jnp.where(right, xl, xr), jnp.where(right, xr, xl)
        part = wd_part(src * 2 + core, bl)
        return copy(part, part, xf_ss, x_rs.at[1, bl], fs, dst * 2 + c)

    def x_wait(kind, bl, parts):
        ref = wdx.at[pl.ds(0, parts)]
        copy(ref, ref, x_ss, x_rs.at[kind, bl], fs, tp).wait_recv()

    def x_step(t):
        b = block_of(t, 1)

        @pl.when(in_half(b))
        def _():
            bl = lax.rem(b, half_z)
            x_wait(0, bl, 2)
            for core in range(2):
                x_forward(bl, core).start()

    def piece(bl, ky, core):
        yt = at_y(ky)
        b = c * half_z + bl
        return copy(
            sendy.at[bl, core, yt], recvy.at[b, y], ry_ss, ry_rs.at[b],
            z * NY + yt, x * 2 + core,
        )

    def compute_step(t):
        b = block_of(t, 1)

        @pl.when(in_half(b))
        def _():
            bl = lax.rem(b, half_z)
            for core, parts in ((0, 6), (1, 4)):
                @pl.when(c == core)
                def _():
                    x_wait(1, bl, parts)

            w = jnp.concatenate([wdx[k * half_z + bl].reshape(NY * 24, 128) for k in range(2 * NX)], axis=1)
            gh = lax.dot_general(w, cotf[...], (((1,), (1,)), ((), ())), preferred_element_type=F32)
            gp = (gh * pret[bl].astype(F32)).astype(BF16)
            gpt[bl] = gp
            for core in range(2):
                @pl.when(c == core)
                def _():
                    own = jnp.dot(gp, inp_ref[...], preferred_element_type=F32)
                    other = jnp.dot(gp, inpx[...], preferred_element_type=F32)
                    sendy[bl, core] = own.reshape(NY, 3, 8, 128).astype(BF16)
                    sendy[bl, 1 - core] = other.reshape(NY, 3, 8, 128).astype(BF16)
            recvy[b, y] = sendy[bl, c, y]
            for ky in range(1, NY):
                for core in range(2):
                    piece(bl, ky, core).start()
            piece(bl, 0, 1 - c).start()

    def z_piece(b):
        return copy(sendz.at[b], recvz.at[z], rz_ss, rz_rs, b * NY + y, tp)

    def reduce_step(t):
        b = block_of(t, 1)
        own = in_half(b)
        for count, when in ((NY - 1, own), (NY, jnp.logical_not(own))):
            @pl.when(when)
            def _():
                ref = recvy.at[b, pl.ds(0, count)]
                copy(ref, ref, ry_ss, ry_rs.at[b], fs, tp).wait_recv()

        total = recvy[b, 0].astype(F32)
        for k in range(1, NY):
            total = total + recvy[b, k].astype(F32)
        sendz[b] = total.astype(BF16)

        @pl.when(t == 0)
        def _():
            recvz[z] = sendz[b]

        @pl.when(t > 0)
        def _():
            z_piece(b).start()

    left, right = xl * 2 + c, xr * 2 + c

    def c_step_one():
        c_wait(0, 2)
        c_fwd(left, 0, xr * 2 + c, 2).start()
        c_fwd(right, 1, xl * 2 + c, 2).start()
        c_fwd(left, 0, sib, 3).start()
        c_fwd(right, 1, sib, 3).start()

    def c_step_half():
        c_wait(1, 2)
        c_fwd(left, 1, sib, 3).start()
        c_fwd(right, 0, sib, 3).start()

    def c_step_two():
        far = xo * 2 + c
        c_wait(2, 2)
        for h in range(2):
            c_fwd(far, h, sib, 3).start()

    def c_step_three():
        c_wait(3, 2 * NX)
        send_inp.wait_recv()

    c_step_one()
    y_parts().wait_recv()

    def run(t, carry):
        hop = lax.div(1 * (t - 1) + 2, 3)
        due = (t >= 1) & (lax.div(3 * hop, 1) == t - 1)
        first = jnp.where(c == 1, jnp.minimum(t, NZ), jnp.maximum(2 * hop - 1, 0))
        last = jnp.where(c == 1, t + 1, jnp.where(due, 2 * hop + 1, 0))
        lax.fori_loop(first, jnp.minimum(last, NZ), gather_step, 0)

        @pl.when(t == 1)
        def _():
            c_step_half()

        @pl.when(t == 3)
        def _():
            c_step_two()

        @pl.when(t == LAG_C)
        def _():
            c_step_three()

        @pl.when((t >= LAG_X) & (t < NZ + LAG_X))
        def _():
            x_step(t - LAG_X)

        @pl.when((t >= LAG_C) & (t < NZ + LAG_C))
        def _():
            compute_step(t - LAG_C)

        @pl.when((t >= LAG_R) & (t < NZ + LAG_R))
        def _():
            reduce_step(t - LAG_R)

        return carry

    lax.fori_loop(0, 20, run, 0)

    @pl.when(c == 1)
    def _():
        copy(wux, wux, x_ss, us_rs, fs, tp).wait_recv()

    def gi_part(core):
        total = None
        for bl in range(half_z):
            gp = jnp.transpose(gpt[bl].astype(F32)).astype(BF16)
            term = jnp.dot(gp, wux[core * half_z + bl].reshape(NY * 24, 128), preferred_element_type=F32)
            total = term if total is None else total + term
        return total

    gisend[...] = gi_part(1 - c)


    def rest(t, carry):
        reduce_step(t)
        return carry

    lax.fori_loop(20 - LAG_R, NZ, rest, 0)
    send_gi = copy(gisend, girecv, g_ss, g_rs, fs, sib)
    send_gi.start()
    own_part = gi_part(c)

    send_gi.wait_recv()
    gi_ref[...] = (own_part + girecv[...]).astype(BF16)

    others = sendz.at[pl.ds(0, NZ - 1)]
    copy(others, others, rz_ss, rz_rs, fs, tp).wait_recv()
    total = recvz[0].astype(F32)
    for k in range(1, NZ):
        total = total + recvz[k].astype(F32)
    scale = 1.0 / math.sqrt(toks * NY * NZ)
    gu_ref[...] = total.reshape(24, 128)[:rows] * scale

    send_inp.wait_send()
    send_gi.wait_send()
    copy(others, others, rz_ss, rz_rs, fs, tp).wait_send()
    for ref, ss in (
        (zr.at[pl.ds(0, 3), pl.ds(0, 2 * NY - 1)], y_ss),
        (cotf.at[:, pl.ds(0, 128 * 7)], c_ss),
        (wdx.at[pl.ds(0, 2 * (NZ - 1))], ring_ss),
        (wdx.at[pl.ds(0, 4 * half_z)], xf_ss),
        (wdx.at[pl.ds(0, 2 * NY - 1), pl.ds(0, 3 * half_z)], ry_ss),
    ):
        copy(ref, ref, ss, g_rs, fs, tp).wait_send()

    @pl.when(c == 1)
    def _():
        copy(wdx, wdx, x_ss, g_rs, fs, tp).wait_send()


def local(cotangent, inputs, pre_act, w_up, w_down):
    toks, cols = cotangent.shape
    rows = w_down.shape[0]
    ff = pre_act.shape[1]
    half = NZ // 2
    hid = 24 * NY
    vmem, dma = pltpu.VMEM, pltpu.SemaphoreType.DMA
    blk = (3 * NY, 8, 128)
    kernel = functools.partial(body, rows)
    return tuple(
        pl.pallas_call(
            kernel,
            out_shape=(
                pltpu.VMEM((toks, cols), BF16),
                pltpu.VMEM((rows, cols), F32),
            ),
            in_specs=[
                pl.BlockSpec(memory_space=pl.ANY),
            ] * 5,
            out_specs=(pl.BlockSpec(memory_space=vmem), pl.BlockSpec(memory_space=vmem)),
            scratch_shapes=[
                vmem((toks, cols), BF16),
                vmem((toks, cols), BF16),
                vmem((rows, cols), BF16),
                vmem((rows, cols), BF16),
                vmem((ff // 2, toks), BF16),
                vmem((toks, 128 * 2 * NX), BF16),
                vmem((toks, 128), BF16),
                vmem((2, 3, 8, 128), BF16),
                vmem((2 * NZ, *blk), BF16),
                vmem((2 * NX * half, *blk), BF16),
                vmem((2 * half, *blk), BF16),
                vmem((half, hid, toks), BF16),
                vmem((half, hid, toks), BF16),
                vmem((half, 2, NY, 3, 8, 128), BF16),
                vmem((NZ, NY, 3, 8, 128), BF16),
                vmem((NZ, 3, 8, 128), BF16),
                vmem((NZ, 3, 8, 128), BF16),
                vmem((toks, 128), F32),
                vmem((toks, 128), F32),
                dma((5,)),
                dma, dma, dma, dma((4,)), dma, dma,
                dma, dma((2 * NZ,)),
                dma, dma, dma((2, half)), dma, dma, dma((NZ,)), dma, dma, dma, dma,
            ],
            compiler_params=pltpu.CompilerParams(collective_id=0, has_side_effects=True),
        )(cotangent, inputs, pre_act.T, w_up, w_down)
    )


def solution(mesh):
    return jax.shard_map(
        local,
        mesh=mesh,
        in_specs=(P("fs", "tp"), P("fs", "tp"), P("fs", None), P("fs", "tp"), P("fs", "tp")),
        out_specs=(P("fs", "tp"), P("fs", "tp")),
        check_vma=False,
    )
```

```python
import functools
import math

import jax
import jax.numpy as jnp
from jax import lax
from jax.experimental import pallas as pl
from jax.experimental.pallas import tpu as pltpu
from jax.sharding import PartitionSpec as P

MESH = pl.DeviceIdType.MESH
F32, BF16 = jnp.float32, jnp.bfloat16
NX, NY, NZ = 4, 8, 12
FAR_FIRST = sorted(range(1, NY), key=lambda k: -min(k, NY - k))
LAG_X, LAG_C, LAG_R = 3, 6, 13


def body(
    rows,
    cot_hbm, inp_hbm, pre_hbm, wu_hbm, wd_hbm,
    gi_ref, gu_ref,
    cot_ref, inp_ref, wu_ref, wd_ref, pre, cotf, inpx, wpad, zr, wdx, wux, pret, gpt, sendy, recvy, sendz, recvz, gisend, girecv,
    load_sem, y_ss, y_rs, c_ss, c_rs, i_ss, i_rs, ring_ss, zr_rs,
    x_ss, xf_ss, x_rs, us_rs, ry_ss, ry_rs, rz_ss, rz_rs, g_ss, g_rs,
):
    fs, tp = lax.axis_index("fs"), lax.axis_index("tp")
    z, y = lax.div(fs, NY), lax.rem(fs, NY)
    x, c = lax.div(tp, 2), lax.rem(tp, 2)
    xr, xl, xo = lax.rem(x + 1, NX), lax.rem(x + NX - 1, NX), lax.rem(x + 2, NX)
    zp, zm = lax.rem(z + 1, NZ), lax.rem(z + NZ - 1, NZ)
    half_z = NZ // 2
    sib = x * 2 + 1 - c
    toks = cot_ref.shape[0]
    tok2 = toks // 2
    hid = rows * NY

    def copy(src, dst, ss, rs, to_fs, to_tp):
        return pltpu.make_async_remote_copy(
            src_ref=src, dst_ref=dst, send_sem=ss, recv_sem=rs,
            device_id=(to_fs, to_tp), device_id_type=MESH,
        )

    barrier = pltpu.get_barrier_semaphore()

    def greet(to_fs, to_tp):
        pl.semaphore_signal(barrier, inc=1, device_id=(to_fs, to_tp), device_id_type=MESH)

    def at_y(k):
        return lax.rem(y + k, NY)

    for k in FAR_FIRST:
        for core in (1, 0):
            greet(z * NY + at_y(k), x * 2 + core)
    greet(zp * NY + y, tp)
    greet(zm * NY + y, tp)
    for core in range(2):
        greet(fs, xr * 2 + core)
        greet(fs, xl * 2 + core)
    greet(fs, sib)

    own_pre = pre_hbm.at[pl.ds(c * (half_z * hid), half_z * hid)]
    loads = [
        pltpu.make_async_copy(src, dst, load_sem.at[k])
        for k, (src, dst) in enumerate(
            ((wd_hbm, wd_ref), (wu_hbm, wu_ref), (cot_hbm, cot_ref), (inp_hbm, inp_ref), (own_pre, pre))
        )
    ]
    for load in loads:
        load.start()

    keep = lax.broadcasted_iota(jnp.int32, (24, rows), 0) == lax.broadcasted_iota(jnp.int32, (24, rows), 1)
    keep = keep.astype(F32).astype(BF16)
    for k, ref in enumerate((wd_ref, wu_ref)):
        loads[k].wait()
        padded = jnp.dot(keep, ref[...], preferred_element_type=F32)
        padded = padded.reshape(3, 8, 128).astype(BF16)
        wpad[k] = padded

    def own_rows(core):
        return zr.at[core * NZ + z, pl.ds(y * 3, 3)]

    own_rows(c)[...] = wpad[1 - c]

    pl.semaphore_wait(barrier, 2 * (NY - 1) + 2 + 4 + 1)

    def y_send(k, w):
        return copy(wpad.at[w], own_rows(c), y_ss, y_rs, z * NY + at_y(k), x * 2 + 1 - w)

    def y_send_sib():
        return copy(wpad.at[c], own_rows(c), y_ss, y_rs, fs, sib)

    for k in FAR_FIRST:
        y_send(k, 0).start()
    y_send_sib().start()

    def lanes(tile):
        return pl.ds(pl.multiple_of(tile * 128, 128), 128)

    def c_part(tile, h):
        return cotf.at[pl.ds(h * tok2, tok2), lanes(tile)]

    def c_own(h, way):
        to = (xr * 2 + c, xl * 2 + c, sib)[way]
        return copy(
            cot_ref.at[pl.ds(h * tok2, tok2)], c_part(tp, h), c_ss, c_rs.at[3 if way == 2 else int(way != h)], fs, to
        )

    def c_fwd(tile, h, to, kind):
        return copy(c_part(tile, h), c_part(tile, h), c_ss, c_rs.at[kind], fs, to)

    def c_wait(kind, parts):
        ref = cotf.at[pl.ds(0, tok2), pl.ds(0, 128 * parts)]
        copy(ref, ref, c_ss, c_rs.at[kind], fs, tp).wait_recv()

    loads[2].wait()
    for h in range(2):
        for way in range(2):
            c_own(h if way == 0 else 1 - h, way).start()
    for k in FAR_FIRST:
        y_send(k, 1).start()
    for h in range(2):
        c_own(h, 2).start()
    loads[3].wait()
    send_inp = copy(inp_ref, inpx, i_ss, i_rs, fs, sib)
    send_inp.start()

    cotf[:, lanes(tp)] = cot_ref[...]

    loads[4].wait()
    iy = lax.broadcasted_iota(jnp.int32, (NY, 24, hid), 0)
    ir = lax.broadcasted_iota(jnp.int32, (NY, 24, hid), 1)
    ik = lax.broadcasted_iota(jnp.int32, (NY, 24, hid), 2)
    pick = ((ik == iy * rows + ir) & (ir < rows)).astype(F32).reshape(NY * 24, hid).astype(BF16)

    def spread(bl, carry):
        part = pre[pl.ds(pl.multiple_of(bl * hid, 16), hid)]
        part = jnp.dot(pick, part, preferred_element_type=F32)
        pret[bl] = (2.0 * jnp.maximum(part, 0.0)).astype(BF16)
        return carry

    lax.fori_loop(0, half_z, spread, 0)

    def y_parts():
        ref = zr.at[pl.ds(0, 3), pl.ds(0, 2 * NY - 1)]
        return copy(ref, ref, y_ss, y_rs, fs, tp)

    def block_of(t, sign):
        s = lax.div(t + 1, 2)
        odd = lax.rem(t, 2) == 1
        return lax.rem(z + NZ + jnp.where(odd, -s, s) * sign, NZ)

    ring_sign = jnp.where(c == 1, 1, -1)
    ring_up, ring_down = jnp.where(c == 1, zp, zm), jnp.where(c == 1, zm, zp)

    def ring_copy(slot, to_z):
        return copy(zr.at[slot], zr.at[slot], ring_ss, zr_rs.at[slot], to_z * NY + y, tp)

    def ring_step(t, slot):
        @pl.when(t > 0)
        def _():
            ring_copy(slot, zp).wait_recv()

        @pl.when(t == 0)
        def _():
            ring_copy(slot, ring_up).start()

        @pl.when(t < NZ - 2)
        def _():
            ring_copy(slot, jnp.where(lax.rem(t, 2) == 1, ring_up, ring_down)).start()

    def wd_part(tile, bl):
        return wdx.at[tile * half_z + bl]

    def via_right(bl, core):
        return lax.rem(bl + core, 2) == 0

    def x_send(k, b, way):
        h, bl = lax.div(b, half_z), lax.rem(b, half_z)
        to = (xr, xl)[way] * 2 + h
        kind = jnp.where(via_right(bl, k) == (way == 0), 0, 1)
        return copy(zr.at[k * NZ + b], wd_part(x * 2 + k, bl), x_ss, x_rs.at[kind, bl], fs, to)

    def in_half(b):
        return lax.div(b, half_z) == c

    def gather_step(t, carry):
        b = block_of(t, ring_sign)
        bl = lax.rem(b, half_z)
        for k in range(2):
            slot = k * NZ + b
            ring_step(t, slot)

            @pl.when(c == 1)
            def _():
                for way in range(2):
                    x_send(k, b, way).start()

                @pl.when(in_half(b))
                def _():
                    wdx[(x * 2 + k) * half_z + bl] = zr[slot]

                @pl.when(jnp.logical_not(in_half(b)))
                def _():
                    copy(zr.at[slot], wd_part(x * 2 + k, bl), xf_ss, x_rs.at[1, bl], fs, sib).start()

            @pl.when(c == 0)
            def _():
                @pl.when(in_half(b))
                def _():
                    wux[k * half_z + bl] = zr[slot]

                @pl.when(jnp.logical_not(in_half(b)))
                def _():
                    copy(zr.at[slot], wux.at[k * half_z + bl], xf_ss, us_rs, fs, sib).start()

        return carry

    def x_forward(bl, core):
        right = via_right(bl, core)
        src, dst = jnp.where(right, xl, xr), jnp.where(right, xr, xl)
        part = wd_part(src * 2 + core, bl)
        return copy(part, part, xf_ss, x_rs.at[1, bl], fs, dst * 2 + c)

    def x_wait(kind, bl, parts):
        ref = wdx.at[pl.ds(0, parts)]
        copy(ref, ref, x_ss, x_rs.at[kind, bl], fs, tp).wait_recv()

    def x_step(t):
        b = block_of(t, 1)

        @pl.when(in_half(b))
        def _():
            bl = lax.rem(b, half_z)
            x_wait(0, bl, 2)
            for core in range(2):
                x_forward(bl, core).start()

    def piece(bl, ky, core):
        yt = at_y(ky)
        b = c * half_z + bl
        return copy(
            sendy.at[bl, core, yt], recvy.at[b, y], ry_ss, ry_rs.at[b],
            z * NY + yt, x * 2 + core,
        )

    def compute_step(t):
        b = block_of(t, 1)

        @pl.when(in_half(b))
        def _():
            bl = lax.rem(b, half_z)
            for core, parts in ((0, 6), (1, 4)):
                @pl.when(c == core)
                def _():
                    x_wait(1, bl, parts)

            w = jnp.concatenate([wdx[k * half_z + bl].reshape(NY * 24, 128) for k in range(2 * NX)], axis=1)
            gh = lax.dot_general(w, cotf[...], (((1,), (1,)), ((), ())), preferred_element_type=F32)
            gp = (gh * pret[bl].astype(F32)).astype(BF16)
            gpt[bl] = gp
            for core in range(2):
                @pl.when(c == core)
                def _():
                    own = jnp.dot(gp, inp_ref[...], preferred_element_type=F32)
                    other = jnp.dot(gp, inpx[...], preferred_element_type=F32)
                    sendy[bl, core] = own.reshape(NY, 3, 8, 128).astype(BF16)
                    sendy[bl, 1 - core] = other.reshape(NY, 3, 8, 128).astype(BF16)
            recvy[b, y] = sendy[bl, c, y]
            for ky in FAR_FIRST:
                for core in range(2):
                    piece(bl, ky, core).start()
            piece(bl, 0, 1 - c).start()

    def z_piece(b):
        return copy(sendz.at[b], recvz.at[z], rz_ss, rz_rs, b * NY + y, tp)

    def reduce_step(t):
        b = block_of(t, 1)
        own = in_half(b)
        for count, when in ((NY - 1, own), (NY, jnp.logical_not(own))):
            @pl.when(when)
            def _():
                ref = recvy.at[b, pl.ds(0, count)]
                copy(ref, ref, ry_ss, ry_rs.at[b], fs, tp).wait_recv()

        total = recvy[b, 0].astype(F32)
        for k in range(1, NY):
            total = total + recvy[b, k].astype(F32)
        sendz[b] = total.astype(BF16)

        @pl.when(t == 0)
        def _():
            recvz[z] = sendz[b]

        @pl.when(t > 0)
        def _():
            z_piece(b).start()

    left, right = xl * 2 + c, xr * 2 + c

    def c_step_one():
        c_wait(0, 2)
        c_fwd(left, 0, xr * 2 + c, 2).start()
        c_fwd(right, 1, xl * 2 + c, 2).start()
        c_fwd(left, 0, sib, 3).start()
        c_fwd(right, 1, sib, 3).start()

    def c_step_half():
        c_wait(1, 2)
        c_fwd(left, 1, sib, 3).start()
        c_fwd(right, 0, sib, 3).start()

    def c_step_two():
        far = xo * 2 + c
        c_wait(2, 2)
        for h in range(2):
            c_fwd(far, h, sib, 3).start()

    def c_step_three():
        c_wait(3, 2 * NX)
        send_inp.wait_recv()

    c_step_one()
    y_parts().wait_recv()

    def run(t, carry):
        hop = lax.div(1 * (t - 1) + 2, 3)
        due = (t >= 1) & (lax.div(3 * hop, 1) == t - 1)
        first = jnp.where(c == 1, jnp.minimum(t, NZ), jnp.maximum(2 * hop - 1, 0))
        last = jnp.where(c == 1, t + 1, jnp.where(due, 2 * hop + 1, 0))
        lax.fori_loop(first, jnp.minimum(last, NZ), gather_step, 0)

        @pl.when(t == 1)
        def _():
            c_step_half()

        @pl.when(t == 3)
        def _():
            c_step_two()

        @pl.when(t == LAG_C)
        def _():
            c_step_three()

        @pl.when((t >= LAG_X) & (t < NZ + LAG_X))
        def _():
            x_step(t - LAG_X)

        @pl.when((t >= LAG_C) & (t < NZ + LAG_C))
        def _():
            compute_step(t - LAG_C)

        @pl.when((t >= LAG_R) & (t < NZ + LAG_R))
        def _():
            reduce_step(t - LAG_R)

        return carry

    lax.fori_loop(0, 20, run, 0)

    @pl.when(c == 1)
    def _():
        copy(wux, wux, x_ss, us_rs, fs, tp).wait_recv()

    def gi_part(core):
        total = None
        for bl in range(half_z):
            gp = jnp.transpose(gpt[bl].astype(F32)).astype(BF16)
            term = jnp.dot(gp, wux[core * half_z + bl].reshape(NY * 24, 128), preferred_element_type=F32)
            total = term if total is None else total + term
        return total

    gisend[...] = gi_part(1 - c)


    def rest(t, carry):
        reduce_step(t)
        return carry

    lax.fori_loop(20 - LAG_R, NZ, rest, 0)
    send_gi = copy(gisend, girecv, g_ss, g_rs, fs, sib)
    send_gi.start()
    own_part = gi_part(c)

    send_gi.wait_recv()
    gi_ref[...] = (own_part + girecv[...]).astype(BF16)

    others = sendz.at[pl.ds(0, NZ - 1)]
    copy(others, others, rz_ss, rz_rs, fs, tp).wait_recv()
    total = recvz[0].astype(F32)
    for k in range(1, NZ):
        total = total + recvz[k].astype(F32)
    scale = 1.0 / math.sqrt(toks * NY * NZ)
    gu_ref[...] = total.reshape(24, 128)[:rows] * scale

    send_inp.wait_send()
    send_gi.wait_send()
    copy(others, others, rz_ss, rz_rs, fs, tp).wait_send()
    for ref, ss in (
        (zr.at[pl.ds(0, 3), pl.ds(0, 2 * NY - 1)], y_ss),
        (cotf.at[:, pl.ds(0, 128 * 7)], c_ss),
        (wdx.at[pl.ds(0, 2 * (NZ - 1))], ring_ss),
        (wdx.at[pl.ds(0, 4 * half_z)], xf_ss),
        (wdx.at[pl.ds(0, 2 * NY - 1), pl.ds(0, 3 * half_z)], ry_ss),
    ):
        copy(ref, ref, ss, g_rs, fs, tp).wait_send()

    @pl.when(c == 1)
    def _():
        copy(wdx, wdx, x_ss, g_rs, fs, tp).wait_send()


def local(cotangent, inputs, pre_act, w_up, w_down):
    toks, cols = cotangent.shape
    rows = w_down.shape[0]
    ff = pre_act.shape[1]
    half = NZ // 2
    hid = 24 * NY
    vmem, dma = pltpu.VMEM, pltpu.SemaphoreType.DMA
    blk = (3 * NY, 8, 128)
    kernel = functools.partial(body, rows)
    return tuple(
        pl.pallas_call(
            kernel,
            out_shape=(
                pltpu.VMEM((toks, cols), BF16),
                pltpu.VMEM((rows, cols), F32),
            ),
            in_specs=[
                pl.BlockSpec(memory_space=pl.ANY),
            ] * 5,
            out_specs=(pl.BlockSpec(memory_space=vmem), pl.BlockSpec(memory_space=vmem)),
            scratch_shapes=[
                vmem((toks, cols), BF16),
                vmem((toks, cols), BF16),
                vmem((rows, cols), BF16),
                vmem((rows, cols), BF16),
                vmem((ff // 2, toks), BF16),
                vmem((toks, 128 * 2 * NX), BF16),
                vmem((toks, 128), BF16),
                vmem((2, 3, 8, 128), BF16),
                vmem((2 * NZ, *blk), BF16),
                vmem((2 * NX * half, *blk), BF16),
                vmem((2 * half, *blk), BF16),
                vmem((half, hid, toks), BF16),
                vmem((half, hid, toks), BF16),
                vmem((half, 2, NY, 3, 8, 128), BF16),
                vmem((NZ, NY, 3, 8, 128), BF16),
                vmem((NZ, 3, 8, 128), BF16),
                vmem((NZ, 3, 8, 128), BF16),
                vmem((toks, 128), F32),
                vmem((toks, 128), F32),
                dma((5,)),
                dma, dma, dma, dma((4,)), dma, dma,
                dma, dma((2 * NZ,)),
                dma, dma, dma((2, half)), dma, dma, dma((NZ,)), dma, dma, dma, dma,
            ],
            compiler_params=pltpu.CompilerParams(collective_id=0, has_side_effects=True),
        )(cotangent, inputs, pre_act.T, w_up, w_down)
    )


def solution(mesh):
    return jax.shard_map(
        local,
        mesh=mesh,
        in_specs=(P("fs", "tp"), P("fs", "tp"), P("fs", None), P("fs", "tp"), P("fs", "tp")),
        out_specs=(P("fs", "tp"), P("fs", "tp")),
        check_vma=False,
    )
```

```python
import functools
import math

import jax
import jax.numpy as jnp
from jax import lax
from jax.experimental import pallas as pl
from jax.experimental.pallas import tpu as pltpu
from jax.sharding import PartitionSpec as P

MESH = pl.DeviceIdType.MESH
F32, BF16 = jnp.float32, jnp.bfloat16
NX, NY, NZ = 4, 8, 12
FAR_FIRST = sorted(range(1, NY), key=lambda k: -min(k, NY - k))
LAG_X, LAG_C, LAG_R = 3, 6, 13


def body(
    rows,
    cot_hbm, inp_hbm, pre_hbm, wu_hbm, wd_hbm,
    gi_ref, gu_ref,
    cot_ref, inp_ref, wu_ref, wd_ref, pre, cotf, inpx, wpad, zr, wdx, wux, pret, gpt, sendy, recvy, sendz, recvz, gisend, girecv,
    load_sem, y_ss, y_rs, c_ss, c_rs, i_ss, i_rs, ring_ss, zr_rs,
    x_ss, xf_ss, x_rs, us_rs, ry_ss, ry_rs, rz_ss, rz_rs, g_ss, g_rs,
):
    fs, tp = lax.axis_index("fs"), lax.axis_index("tp")
    z, y = lax.div(fs, NY), lax.rem(fs, NY)
    x, c = lax.div(tp, 2), lax.rem(tp, 2)
    xr, xl, xo = lax.rem(x + 1, NX), lax.rem(x + NX - 1, NX), lax.rem(x + 2, NX)
    zp, zm = lax.rem(z + 1, NZ), lax.rem(z + NZ - 1, NZ)
    half_z = NZ // 2
    sib = x * 2 + 1 - c
    toks = cot_ref.shape[0]
    tok2 = toks // 2
    hid = rows * NY

    def copy(src, dst, ss, rs, to_fs, to_tp):
        return pltpu.make_async_remote_copy(
            src_ref=src, dst_ref=dst, send_sem=ss, recv_sem=rs,
            device_id=(to_fs, to_tp), device_id_type=MESH,
        )

    own_pre = pre_hbm.at[pl.ds(c * (half_z * hid), half_z * hid)]
    loads = [
        pltpu.make_async_copy(src, dst, load_sem.at[k])
        for k, (src, dst) in enumerate(
            ((wd_hbm, wd_ref), (wu_hbm, wu_ref), (cot_hbm, cot_ref), (inp_hbm, inp_ref), (own_pre, pre))
        )
    ]
    for load in loads[:2]:
        load.start()

    barrier = pltpu.get_barrier_semaphore()

    def greet(to_fs, to_tp):
        pl.semaphore_signal(barrier, inc=1, device_id=(to_fs, to_tp), device_id_type=MESH)

    def at_y(k):
        return lax.rem(y + k, NY)

    for k in FAR_FIRST:
        for core in (1, 0):
            greet(z * NY + at_y(k), x * 2 + core)
    greet(zp * NY + y, tp)
    greet(zm * NY + y, tp)
    for core in range(2):
        greet(fs, xr * 2 + core)
        greet(fs, xl * 2 + core)
    greet(fs, sib)

    for load in loads[2:]:
        load.start()

    keep = lax.broadcasted_iota(jnp.int32, (24, rows), 0) == lax.broadcasted_iota(jnp.int32, (24, rows), 1)
    keep = keep.astype(F32).astype(BF16)
    for k, ref in enumerate((wd_ref, wu_ref)):
        loads[k].wait()
        padded = jnp.dot(keep, ref[...], preferred_element_type=F32)
        padded = padded.reshape(3, 8, 128).astype(BF16)
        wpad[k] = padded

    def own_rows(core):
        return zr.at[core * NZ + z, pl.ds(y * 3, 3)]

    own_rows(c)[...] = wpad[1 - c]

    pl.semaphore_wait(barrier, 2 * (NY - 1) + 2 + 4 + 1)

    def y_send(k, w):
        return copy(wpad.at[w], own_rows(c), y_ss, y_rs, z * NY + at_y(k), x * 2 + 1 - w)

    def y_send_sib():
        return copy(wpad.at[c], own_rows(c), y_ss, y_rs, fs, sib)

    for k in FAR_FIRST:
        y_send(k, 0).start()
    y_send_sib().start()

    def lanes(tile):
        return pl.ds(pl.multiple_of(tile * 128, 128), 128)

    def c_part(tile, h):
        return cotf.at[pl.ds(h * tok2, tok2), lanes(tile)]

    def c_own(h, way):
        to = (xr * 2 + c, xl * 2 + c, sib)[way]
        return copy(
            cot_ref.at[pl.ds(h * tok2, tok2)], c_part(tp, h), c_ss, c_rs.at[3 if way == 2 else int(way != h)], fs, to
        )

    def c_fwd(tile, h, to, kind):
        return copy(c_part(tile, h), c_part(tile, h), c_ss, c_rs.at[kind], fs, to)

    def c_wait(kind, parts):
        ref = cotf.at[pl.ds(0, tok2), pl.ds(0, 128 * parts)]
        copy(ref, ref, c_ss, c_rs.at[kind], fs, tp).wait_recv()

    loads[2].wait()
    for h in range(2):
        for way in range(2):
            c_own(h if way == 0 else 1 - h, way).start()
    for k in FAR_FIRST:
        y_send(k, 1).start()
    for h in range(2):
        c_own(h, 2).start()
    loads[3].wait()
    send_inp = copy(inp_ref, inpx, i_ss, i_rs, fs, sib)
    send_inp.start()

    cotf[:, lanes(tp)] = cot_ref[...]

    loads[4].wait()
    iy = lax.broadcasted_iota(jnp.int32, (NY, 24, hid), 0)
    ir = lax.broadcasted_iota(jnp.int32, (NY, 24, hid), 1)
    ik = lax.broadcasted_iota(jnp.int32, (NY, 24, hid), 2)
    pick = ((ik == iy * rows + ir) & (ir < rows)).astype(F32).reshape(NY * 24, hid).astype(BF16)

    def spread(bl, carry):
        part = pre[pl.ds(pl.multiple_of(bl * hid, 16), hid)]
        part = jnp.dot(pick, part, preferred_element_type=F32)
        pret[bl] = (2.0 * jnp.maximum(part, 0.0)).astype(BF16)
        return carry

    lax.fori_loop(0, half_z, spread, 0)

    def y_parts():
        ref = zr.at[pl.ds(0, 3), pl.ds(0, 2 * NY - 1)]
        return copy(ref, ref, y_ss, y_rs, fs, tp)

    def block_of(t, sign):
        s = lax.div(t + 1, 2)
        odd = lax.rem(t, 2) == 1
        return lax.rem(z + NZ + jnp.where(odd, -s, s) * sign, NZ)

    ring_sign = jnp.where(c == 1, 1, -1)
    ring_up, ring_down = jnp.where(c == 1, zp, zm), jnp.where(c == 1, zm, zp)

    def ring_copy(slot, to_z):
        return copy(zr.at[slot], zr.at[slot], ring_ss, zr_rs.at[slot], to_z * NY + y, tp)

    def ring_step(t, slot):
        @pl.when(t > 0)
        def _():
            ring_copy(slot, zp).wait_recv()

        @pl.when(t == 0)
        def _():
            ring_copy(slot, ring_up).start()

        @pl.when(t < NZ - 2)
        def _():
            ring_copy(slot, jnp.where(lax.rem(t, 2) == 1, ring_up, ring_down)).start()

    def wd_part(tile, bl):
        return wdx.at[tile * half_z + bl]

    def via_right(bl, core):
        return lax.rem(bl + core, 2) == 0

    def x_send(k, b, way):
        h, bl = lax.div(b, half_z), lax.rem(b, half_z)
        to = (xr, xl)[way] * 2 + h
        kind = jnp.where(via_right(bl, k) == (way == 0), 0, 1)
        return copy(zr.at[k * NZ + b], wd_part(x * 2 + k, bl), x_ss, x_rs.at[kind, bl], fs, to)

    def in_half(b):
        return lax.div(b, half_z) == c

    def gather_step(t, carry):
        b = block_of(t, ring_sign)
        bl = lax.rem(b, half_z)
        for k in range(2):
            slot = k * NZ + b
            ring_step(t, slot)

            @pl.when(c == 1)
            def _():
                for way in range(2):
                    x_send(k, b, way).start()

                @pl.when(in_half(b))
                def _():
                    wdx[(x * 2 + k) * half_z + bl] = zr[slot]

                @pl.when(jnp.logical_not(in_half(b)))
                def _():
                    copy(zr.at[slot], wd_part(x * 2 + k, bl), xf_ss, x_rs.at[1, bl], fs, sib).start()

            @pl.when(c == 0)
            def _():
                @pl.when(in_half(b))
                def _():
                    wux[k * half_z + bl] = zr[slot]

                @pl.when(jnp.logical_not(in_half(b)))
                def _():
                    copy(zr.at[slot], wux.at[k * half_z + bl], xf_ss, us_rs, fs, sib).start()

        return carry

    def x_forward(bl, core):
        right = via_right(bl, core)
        src, dst = jnp.where(right, xl, xr), jnp.where(right, xr, xl)
        part = wd_part(src * 2 + core, bl)
        return copy(part, part, xf_ss, x_rs.at[1, bl], fs, dst * 2 + c)

    def x_wait(kind, bl, parts):
        ref = wdx.at[pl.ds(0, parts)]
        copy(ref, ref, x_ss, x_rs.at[kind, bl], fs, tp).wait_recv()

    def x_step(t):
        b = block_of(t, 1)

        @pl.when(in_half(b))
        def _():
            bl = lax.rem(b, half_z)
            x_wait(0, bl, 2)
            for core in range(2):
                x_forward(bl, core).start()

    def piece(bl, ky, core):
        yt = at_y(ky)
        b = c * half_z + bl
        return copy(
            sendy.at[bl, core, yt], recvy.at[b, y], ry_ss, ry_rs.at[b],
            z * NY + yt, x * 2 + core,
        )

    def compute_step(t):
        b = block_of(t, 1)

        @pl.when(in_half(b))
        def _():
            bl = lax.rem(b, half_z)
            for core, parts in ((0, 6), (1, 4)):
                @pl.when(c == core)
                def _():
                    x_wait(1, bl, parts)

            w = jnp.concatenate([wdx[k * half_z + bl].reshape(NY * 24, 128) for k in range(2 * NX)], axis=1)
            gh = lax.dot_general(w, cotf[...], (((1,), (1,)), ((), ())), preferred_element_type=F32)
            gp = (gh * pret[bl].astype(F32)).astype(BF16)
            gpt[bl] = gp
            for core in range(2):
                @pl.when(c == core)
                def _():
                    own = jnp.dot(gp, inp_ref[...], preferred_element_type=F32)
                    other = jnp.dot(gp, inpx[...], preferred_element_type=F32)
                    sendy[bl, core] = own.reshape(NY, 3, 8, 128).astype(BF16)
                    sendy[bl, 1 - core] = other.reshape(NY, 3, 8, 128).astype(BF16)
            recvy[b, y] = sendy[bl, c, y]
            for ky in FAR_FIRST:
                for core in range(2):
                    piece(bl, ky, core).start()
            piece(bl, 0, 1 - c).start()

    def z_piece(b):
        return copy(sendz.at[b], recvz.at[z], rz_ss, rz_rs, b * NY + y, tp)

    def reduce_step(t):
        b = block_of(t, 1)
        own = in_half(b)
        for count, when in ((NY - 1, own), (NY, jnp.logical_not(own))):
            @pl.when(when)
            def _():
                ref = recvy.at[b, pl.ds(0, count)]
                copy(ref, ref, ry_ss, ry_rs.at[b], fs, tp).wait_recv()

        total = recvy[b, 0].astype(F32)
        for k in range(1, NY):
            total = total + recvy[b, k].astype(F32)
        sendz[b] = total.astype(BF16)

        @pl.when(t == 0)
        def _():
            recvz[z] = sendz[b]

        @pl.when(t > 0)
        def _():
            z_piece(b).start()

    left, right = xl * 2 + c, xr * 2 + c

    def c_step_one():
        c_wait(0, 2)
        c_fwd(left, 0, xr * 2 + c, 2).start()
        c_fwd(right, 1, xl * 2 + c, 2).start()
        c_fwd(left, 0, sib, 3).start()
        c_fwd(right, 1, sib, 3).start()

    def c_step_half():
        c_wait(1, 2)
        c_fwd(left, 1, sib, 3).start()
        c_fwd(right, 0, sib, 3).start()

    def c_step_two():
        far = xo * 2 + c
        c_wait(2, 2)
        for h in range(2):
            c_fwd(far, h, sib, 3).start()

    def c_step_three():
        c_wait(3, 2 * NX)
        send_inp.wait_recv()

    c_step_one()
    y_parts().wait_recv()

    def run(t, carry):
        hop = lax.div(1 * (t - 1) + 2, 3)
        due = (t >= 1) & (lax.div(3 * hop, 1) == t - 1)
        first = jnp.where(c == 1, jnp.minimum(t, NZ), jnp.maximum(2 * hop - 1, 0))
        last = jnp.where(c == 1, t + 1, jnp.where(due, 2 * hop + 1, 0))
        lax.fori_loop(first, jnp.minimum(last, NZ), gather_step, 0)

        @pl.when(t == 1)
        def _():
            c_step_half()

        @pl.when(t == 3)
        def _():
            c_step_two()

        @pl.when(t == LAG_C)
        def _():
            c_step_three()

        @pl.when((t >= LAG_X) & (t < NZ + LAG_X))
        def _():
            x_step(t - LAG_X)

        @pl.when((t >= LAG_C) & (t < NZ + LAG_C))
        def _():
            compute_step(t - LAG_C)

        @pl.when((t >= LAG_R) & (t < NZ + LAG_R))
        def _():
            reduce_step(t - LAG_R)

        return carry

    lax.fori_loop(0, 20, run, 0)

    @pl.when(c == 1)
    def _():
        copy(wux, wux, x_ss, us_rs, fs, tp).wait_recv()

    def gi_part(core):
        total = None
        for bl in range(half_z):
            gp = jnp.transpose(gpt[bl].astype(F32)).astype(BF16)
            term = jnp.dot(gp, wux[core * half_z + bl].reshape(NY * 24, 128), preferred_element_type=F32)
            total = term if total is None else total + term
        return total

    gisend[...] = gi_part(1 - c)


    def rest(t, carry):
        reduce_step(t)
        return carry

    lax.fori_loop(20 - LAG_R, NZ, rest, 0)
    send_gi = copy(gisend, girecv, g_ss, g_rs, fs, sib)
    send_gi.start()
    own_part = gi_part(c)

    send_gi.wait_recv()
    gi_ref[...] = (own_part + girecv[...]).astype(BF16)

    others = sendz.at[pl.ds(0, NZ - 1)]
    copy(others, others, rz_ss, rz_rs, fs, tp).wait_recv()
    total = recvz[0].astype(F32)
    for k in range(1, NZ):
        total = total + recvz[k].astype(F32)
    scale = 1.0 / math.sqrt(toks * NY * NZ)
    gu_ref[...] = total.reshape(24, 128)[:rows] * scale

    send_inp.wait_send()
    send_gi.wait_send()
    copy(others, others, rz_ss, rz_rs, fs, tp).wait_send()
    for ref, ss in (
        (zr.at[pl.ds(0, 3), pl.ds(0, 2 * NY - 1)], y_ss),
        (cotf.at[:, pl.ds(0, 128 * 7)], c_ss),
        (wdx.at[pl.ds(0, 2 * (NZ - 1))], ring_ss),
        (wdx.at[pl.ds(0, 4 * half_z)], xf_ss),
        (wdx.at[pl.ds(0, 2 * NY - 1), pl.ds(0, 3 * half_z)], ry_ss),
    ):
        copy(ref, ref, ss, g_rs, fs, tp).wait_send()

    @pl.when(c == 1)
    def _():
        copy(wdx, wdx, x_ss, g_rs, fs, tp).wait_send()


def local(cotangent, inputs, pre_act, w_up, w_down):
    toks, cols = cotangent.shape
    rows = w_down.shape[0]
    ff = pre_act.shape[1]
    half = NZ // 2
    hid = 24 * NY
    vmem, dma = pltpu.VMEM, pltpu.SemaphoreType.DMA
    blk = (3 * NY, 8, 128)
    kernel = functools.partial(body, rows)
    return tuple(
        pl.pallas_call(
            kernel,
            out_shape=(
                pltpu.VMEM((toks, cols), BF16),
                pltpu.VMEM((rows, cols), F32),
            ),
            in_specs=[
                pl.BlockSpec(memory_space=pl.ANY),
            ] * 5,
            out_specs=(pl.BlockSpec(memory_space=vmem), pl.BlockSpec(memory_space=vmem)),
            scratch_shapes=[
                vmem((toks, cols), BF16),
                vmem((toks, cols), BF16),
                vmem((rows, cols), BF16),
                vmem((rows, cols), BF16),
                vmem((ff // 2, toks), BF16),
                vmem((toks, 128 * 2 * NX), BF16),
                vmem((toks, 128), BF16),
                vmem((2, 3, 8, 128), BF16),
                vmem((2 * NZ, *blk), BF16),
                vmem((2 * NX * half, *blk), BF16),
                vmem((2 * half, *blk), BF16),
                vmem((half, hid, toks), BF16),
                vmem((half, hid, toks), BF16),
                vmem((half, 2, NY, 3, 8, 128), BF16),
                vmem((NZ, NY, 3, 8, 128), BF16),
                vmem((NZ, 3, 8, 128), BF16),
                vmem((NZ, 3, 8, 128), BF16),
                vmem((toks, 128), F32),
                vmem((toks, 128), F32),
                dma((5,)),
                dma, dma, dma, dma((4,)), dma, dma,
                dma, dma((2 * NZ,)),
                dma, dma, dma((2, half)), dma, dma, dma((NZ,)), dma, dma, dma, dma,
            ],
            compiler_params=pltpu.CompilerParams(collective_id=0, has_side_effects=True),
        )(cotangent, inputs, pre_act.T, w_up, w_down)
    )


def solution(mesh):
    return jax.shard_map(
        local,
        mesh=mesh,
        in_specs=(P("fs", "tp"), P("fs", "tp"), P("fs", None), P("fs", "tp"), P("fs", "tp")),
        out_specs=(P("fs", "tp"), P("fs", "tp")),
        check_vma=False,
    )
```
